256 devices in a mesh: sp: 64 (over z, x, core), tp: 4 (over y).
Axes of the slice: x: 4, y: 4, z: 8, core: 2. Of those that a mesh axis runs over, the one named last changes fastest.
Arguments:
- receptance: bfloat16 [8192, 1024], P('sp', 'tp'), may hold values from -6 to 6
- key_by_head: bfloat16 [8192, 1024], P('sp', 'tp'), may hold values from -6 to 6
- value_head_rows: bfloat16 [8192, 1024], P('sp', 'tp'), may hold values from -6 to 6
- decay_preact: bfloat16 [8192, 1024], P('sp', 'tp'), may hold values from -13 to -0.5
- correction_preact: bfloat16 [8192, 1024], P('sp', 'tp'), may hold values from -7 to 3
- result_sigmoid_factor: bfloat16 [8192, 1024], P('sp', 'tp'), may hold values from -6 to 6
- key_rate_mixing: float32 [1024], P('tp'), may hold values from 0.3 to 0.9
- diagonal_current_factor: float32 [1024], P('tp'), may hold values from -0.6 to 0.6
- per_head_gain: float32 [1024], P('tp'), may hold values from 0.1 to 1.9
- per_head_bias: float32 [1024], P('tp'), may hold values from -1.5 to 1.5
- output_matrix: bfloat16 [1024, 2048], P('tp'), may hold values from -0.1875 to 0.1875
- residual: bfloat16 [8192, 2048], P('sp'), may hold values from -6 to 6
- expert_norm_gain: float32 [2048], replicated, may hold values from 0.1 to 1.9
- routes: int32 [8192, 8], P('sp'), may hold values from 0 to 255, all different within a row; in each aligned block of 128 rows (0 to 127, 128 to 255, ...) at most 6 rows name the same one
- chosen_expert_weight: float32 [8192, 8], P('sp'), may hold values from 0.05 to 0.6
- routed_gate_weight: bfloat16 [256, 2048, 512], P(('sp', 'tp')), may hold values from -0.125 to 0.125
- routed_up_weight: bfloat16 [256, 2048, 512], P(('sp', 'tp')), may hold values from -0.125 to 0.125
- routed_down_weight: bfloat16 [256, 512, 2048], P(('sp', 'tp')), may hold values from -0.25 to 0.25
- common_gate_weight: bfloat16 [2048, 512], P(None, 'tp'), may hold values from -0.125 to 0.125
- common_up_weight: bfloat16 [2048, 512], P(None, 'tp'), may hold values from -0.125 to 0.125
- common_down_weight: bfloat16 [512, 2048], P('tp'), may hold values from -0.25 to 0.25
Outputs:
- layer_out: bfloat16 [8192, 2048], P('sp', 'tp')
The draws below stay inside these ranges and needn't reach their ends.
Inputs may be any that keep to these rules, and one draw needn't show every extreme that they name: `routes`: each row names 8 different experts; in each aligned block of 128 rows no expert is named by more than 6 rows.
All inputs are finite; a program needn't handle non-finite values.
Results may differ from the reference program's by a relative error of at most 0.018.
Values may be sent and summed in bfloat16 or wider, within the bound.
No kernel may reach another device: no remote copies, remote signals or barrier semaphores. Data moves between devices by JAX's collectives and lax.ppermute only.
A program may use at most 64 MiB of HBM per device.

```python
import math
import jax
import jax.numpy as jnp
import numpy as np
from jax import lax

D = 2048
HEADS = 16
CHANNEL_SPAN = 64
FF = 512
TOP_K = 8
TOK_DEV = 128
INNER_WIDTH = 1024
EXPERTS = 256
TOKENS = 8192
CAP = 6
N_SP = 64


def head_pattern(key):
    chance = 0.5
    slow_heads = jax.random.bernoulli(jax.random.fold_in(key, 11), chance, (HEADS,))
    return jnp.repeat(slow_heads, CHANNEL_SPAN)


def draw_decay_preact(key, part):
    slow_cols = head_pattern(key)
    jitter = jax.random.uniform(jax.random.fold_in(key, 21), (TOKENS, INNER_WIDTH), jnp.float32, -1.5, 1.5)
    block_count = TOKENS // TOK_DEV
    offsets = jax.random.uniform(jax.random.fold_in(key, 22), (block_count, 1, INNER_WIDTH), jnp.float32, -0.5, 0.5)
    offsets = jnp.broadcast_to(offsets, (block_count, TOK_DEV, INNER_WIDTH)).reshape(TOKENS, INNER_WIDTH)
    base_level = jnp.where(slow_cols, -11.0, -2.5)
    return (base_level[None, :] + jitter + offsets).astype(jnp.bfloat16)


def draw_correction_preact(key, part):
    slow_cols = head_pattern(key)
    fast_part = jax.random.uniform(jax.random.fold_in(key, 31), (TOKENS, INNER_WIDTH), jnp.float32, -3.0, 3.0)
    slow_part = jax.random.uniform(jax.random.fold_in(key, 32), (TOKENS, INNER_WIDTH), jnp.float32, -7.0, -5.0)
    return jnp.where(slow_cols[None, :], slow_part, fast_part).astype(jnp.bfloat16)


def block_levels(stream_key, shape, split, low, top_value):
    loudness = 1.0
    for axis_at, blocks in split:
        heights = jax.random.uniform(jax.random.fold_in(jax.random.fold_in(stream_key, 6), axis_at), (blocks,), jnp.float32, low / len(split), top_value / len(split))
        loudness = loudness * jnp.repeat(jnp.exp(heights), shape[axis_at] // blocks).reshape((-1,) + (1,) * (len(shape) - 1 - axis_at))
    return loudness


def assign_block(stream_key, own, number, rows, count, top, limit, skew):
    order = jax.random.permutation(stream_key, count)
    crowded, common = shares(count, rows * top, limit, skew, True), shares(count, rows * top, limit, skew, False)
    places = jnp.arange(count)

    def named(sizes, rotation):
        used = int((sizes > 0).sum())
        fixed = max(1, used // 4)
        passed = fixed + (places - fixed + rotation * (used - fixed)) % max(1, count - fixed)
        return jnp.zeros((count,), jnp.int32).at[order[jnp.where(places < fixed, places, passed)]].set(jnp.asarray(sizes, jnp.int32))

    sizes = jnp.where(number % 4 == 0, named(crowded, number // 4), named(common, number - number // 4 - 1))
    mixed = jax.random.permutation(jax.random.fold_in(own, 3), count)
    donor, taker = mixed[0:count // 2 * 2:2], mixed[1:count // 2 * 2:2]
    slack = jnp.minimum(sizes[donor] - 1, limit - sizes[taker]) // 2
    slack = jnp.where((donor == order[0]) | (taker == order[0]) | (sizes[taker] == 0), 0, jnp.maximum(slack, 0))
    passed = jax.random.randint(jax.random.fold_in(own, 4), (count // 2,), 0, 1 << 20) % (slack + 1)
    sizes = sizes.at[donor].add(-passed).at[taker].add(passed)
    members = jnp.searchsorted(jnp.cumsum(sizes), jnp.arange(rows * top), side="right").astype(jnp.int32)
    table = members.reshape(top, rows).T
    table = table[jax.random.permutation(jax.random.fold_in(own, 1), rows)]
    rotation = jax.random.randint(jax.random.fold_in(own, 2), (rows, 1), 0, top)
    return jnp.take_along_axis(table, (jnp.arange(top)[None, :] + rotation) % top, axis=1)


def shares(count, total, reach, skew, full):
    weights = [(1 << 20) // math.isqrt(rank ** skew) + 1 for rank in range(1, count + 1)]
    largest = reach if full else min(reach, max(-(-total // count), total * weights[0] // sum(weights)))
    least = 1 if total - largest >= count - 1 else 0
    given, spare = [largest] + [least] * (count - 1), total - largest - least * (count - 1)
    while spare > 0:
        movable = [i for i in range(1, count) if given[i] < largest] or [i for i in range(1, count) if given[i] < reach]
        mass, remaining = sum([weights[i] for i in movable]), spare
        for i in movable:
            more = min(reach - given[i], max(1, remaining * weights[i] // mass), spare)
            given[i] = given[i] + more
            spare = spare - more
    return np.array(given)


def noise(own_key, dims, width, bound, split=(), kind=jnp.bfloat16):
    values = jax.random.normal(own_key, dims, jnp.float32) * width
    if len(split) > 0:
        values = block_levels(own_key, dims, split, -0.22, 0.18) * values
    return jnp.clip(values, min=-bound, max=bound).astype(kind)


def setup_inputs(seed: int = 0) -> dict:
    keys = jax.random.split(jax.random.key(seed), 22)
    receptance = noise(keys[0], (TOKENS, INNER_WIDTH), 1.0, 6.0, ((0, 64), (1, 4)))
    key_by_head = noise(keys[1], (TOKENS, INNER_WIDTH), 1.0, 6.0, ((0, 64), (1, 4)))
    value_head_rows = noise(keys[2], (TOKENS, INNER_WIDTH), 1.0, 6.0, ((0, 64), (1, 4)))
    decay_preact = draw_decay_preact(jax.random.fold_in(keys[21], 71), 0)
    correction_preact = draw_correction_preact(jax.random.fold_in(keys[21], 71), 0)
    result_sigmoid_factor = noise(keys[5], (TOKENS, INNER_WIDTH), 1.0, 6.0, ((0, 64), (1, 4)))
    key_rate_mixing = jnp.clip(0.3 + 0.59999996 * jax.random.uniform(keys[6], (INNER_WIDTH,), jnp.float32) ** block_levels(keys[6], (INNER_WIDTH,), ((0, 4),), -0.2, 0.2), 0.3, 0.9)
    diagonal_current_factor = noise(keys[7], (INNER_WIDTH,), 0.12, 0.6, ((0, 4),), jnp.float32)
    per_head_gain = jnp.clip(1.0 + 0.18 * jax.random.normal(keys[8], (INNER_WIDTH,), jnp.float32), 0.1, 1.9)
    per_head_bias = noise(keys[9], (INNER_WIDTH,), 0.3, 1.5, ((0, 4),), jnp.float32)
    output_matrix = noise(keys[10], (INNER_WIDTH, D), INNER_WIDTH ** -0.5, 0.1875, ((0, 4),))
    residual = noise(keys[11], (TOKENS, D), 1.0, 6.0, ((0, 64),))
    expert_norm_gain = jnp.clip(1.0 + 0.18 * jax.random.normal(keys[12], (D,), jnp.float32), 0.1, 1.9)
    routes_keys = jax.random.split(jax.random.fold_in(keys[13], 1), TOKENS // TOK_DEV)
    routes_turns = jax.random.permutation(jax.random.fold_in(keys[13], 3), TOKENS // TOK_DEV)
    routes = jax.vmap(lambda own, number: assign_block(jax.random.fold_in(keys[13], 2), own, number, TOK_DEV, EXPERTS, TOP_K, CAP, 2))(routes_keys, routes_turns).reshape((TOKENS, TOP_K))
    chosen_expert_weight = jnp.clip(0.05 + 0.55 * jax.random.uniform(keys[14], (TOKENS, TOP_K), jnp.float32) ** block_levels(keys[14], (TOKENS, TOP_K), ((0, 64),), -0.2, 0.2), 0.05, 0.6)
    routed_gate_weight = noise(keys[15], (EXPERTS, D, FF), D ** -0.5, 0.125, ((0, 256),))
    routed_up_weight = noise(keys[16], (EXPERTS, D, FF), D ** -0.5, 0.125, ((0, 256),))
    routed_down_weight = noise(keys[17], (EXPERTS, FF, D), FF ** -0.5, 0.25, ((0, 256),))
    common_gate_weight = noise(keys[18], (D, FF), D ** -0.5, 0.125, ((1, 4),))
    common_up_weight = noise(keys[19], (D, FF), D ** -0.5, 0.125, ((1, 4),))
    common_down_weight = noise(keys[20], (FF, D), FF ** -0.5, 0.25, ((0, 4),))
    return {"receptance": receptance, "key_by_head": key_by_head, "value_head_rows": value_head_rows, "decay_preact": decay_preact, "correction_preact": correction_preact, "result_sigmoid_factor": result_sigmoid_factor, "key_rate_mixing": key_rate_mixing, "diagonal_current_factor": diagonal_current_factor, "per_head_gain": per_head_gain, "per_head_bias": per_head_bias, "output_matrix": output_matrix, "residual": residual, "expert_norm_gain": expert_norm_gain, "routes": routes, "chosen_expert_weight": chosen_expert_weight, "routed_gate_weight": routed_gate_weight, "routed_up_weight": routed_up_weight, "routed_down_weight": routed_down_weight, "common_gate_weight": common_gate_weight, "common_up_weight": common_up_weight, "common_down_weight": common_down_weight}


NORM_EPS = 1e-06
GROUP_EPS = 0.00064
HIGHEST = lax.Precision.HIGHEST

def partition_channels(source, head_size):
    row_count, col_count = source.shape
    return source.astype(jnp.float32).reshape(row_count, col_count // head_size, head_size)

def prepare(receptance, key_by_head, value_head_rows, decay_preact, correction_preact, key_rate_mixing):
    key_rows = partition_channels(key_by_head, CHANNEL_SPAN)
    learning = jax.nn.sigmoid(partition_channels(correction_preact, CHANNEL_SPAN))
    length = jnp.sqrt(lax.optimization_barrier(jnp.sum(key_rows * key_rows, axis=-1, keepdims=True)))
    unit_keys = key_rows / jnp.maximum(length, 1.0)
    mix_rows = key_rate_mixing.astype(jnp.float32).reshape(1, key_rows.shape[1], CHANNEL_SPAN)
    interpolated_lookup_vectors = key_rows * (1.0 + (learning - 1.0) * mix_rows)
    log_decay = -jnp.exp(-jax.nn.softplus(-partition_channels(decay_preact, CHANNEL_SPAN)) - 0.5)
    return (partition_channels(receptance, CHANNEL_SPAN), interpolated_lookup_vectors, partition_channels(value_head_rows, CHANNEL_SPAN), log_decay, unit_keys, learning)

def finalize(state_readout, query_vectors_partitioned, interpolated_lookup_vectors, content_vectors_partitioned, per_head_gain, per_head_bias, diagonal_current_factor, result_sigmoid_factor):
    shard_attention_count = state_readout.shape[1]
    average = lax.optimization_barrier(jnp.mean(state_readout, axis=-1, keepdims=True))
    centred = state_readout - average
    variance = lax.optimization_barrier(jnp.mean(centred * centred, axis=-1, keepdims=True))
    standardized_channels = centred * lax.rsqrt(variance + GROUP_EPS)
    standardized_channels = standardized_channels * per_head_gain.astype(jnp.float32).reshape(1, shard_attention_count, CHANNEL_SPAN) + per_head_bias.astype(jnp.float32).reshape(1, shard_attention_count, CHANNEL_SPAN)
    diagonal_extra_contribution = lax.optimization_barrier(jnp.sum(query_vectors_partitioned * interpolated_lookup_vectors * diagonal_current_factor.astype(jnp.float32).reshape(1, shard_attention_count, CHANNEL_SPAN), axis=-1, keepdims=True)) * content_vectors_partitioned
    concatenated_channels = (standardized_channels + diagonal_extra_contribution) * partition_channels(result_sigmoid_factor, CHANNEL_SPAN)
    return concatenated_channels.reshape(state_readout.shape[0], shard_attention_count * CHANNEL_SPAN).astype(jnp.bfloat16)

def expert_apply(rows_in, gate_weight, up_weight, down_weight):
    gate_part = jnp.dot(rows_in, gate_weight, preferred_element_type=jnp.float32)
    up_part = jnp.dot(rows_in, up_weight, preferred_element_type=jnp.float32)
    hidden = (jax.nn.silu(gate_part) * up_part).astype(jnp.bfloat16)
    return jnp.dot(hidden, down_weight, preferred_element_type=jnp.float32)

def reference(receptance, key_by_head, value_head_rows, decay_preact, correction_preact, result_sigmoid_factor, key_rate_mixing, diagonal_current_factor, per_head_gain, per_head_bias, output_matrix, residual, expert_norm_gain, routes, chosen_expert_weight, routed_gate_weight, routed_up_weight, routed_down_weight, common_gate_weight, common_up_weight, common_down_weight):
    query_vectors_partitioned, interpolated_lookup_vectors, content_vectors_partitioned, log_decay, unit_keys, learning = prepare(receptance, key_by_head, value_head_rows, decay_preact, correction_preact, key_rate_mixing)
    decay = jnp.exp(log_decay)

    def advance(memory, inputs):
        recept_now, key_now, value_now, decay_now, unit_now, learn_now = inputs
        erased = jnp.einsum('hij,hj->hi', memory, -unit_now, precision=HIGHEST)
        memory = memory * decay_now[:, None, :] + erased[:, :, None] * (unit_now * learn_now)[:, None, :] + value_now[:, :, None] * key_now[:, None, :]
        return (memory, jnp.einsum('hij,hj->hi', memory, recept_now, precision=HIGHEST))
    start_memory = jnp.zeros((HEADS, CHANNEL_SPAN, CHANNEL_SPAN), jnp.float32)
    final_memory, state_readout = lax.scan(advance, start_memory, (query_vectors_partitioned, interpolated_lookup_vectors, content_vectors_partitioned, decay, unit_keys, learning))
    blended_heads = finalize(state_readout, query_vectors_partitioned, interpolated_lookup_vectors, content_vectors_partitioned, per_head_gain, per_head_bias, diagonal_current_factor, result_sigmoid_factor)
    projected = jnp.dot(blended_heads, output_matrix, preferred_element_type=jnp.float32)
    middle = (residual.astype(jnp.float32) + projected).astype(jnp.bfloat16)
    middle_full = middle.astype(jnp.float32)
    row_scale = lax.rsqrt(lax.optimization_barrier(jnp.mean(middle_full * middle_full, axis=-1, keepdims=True)) + NORM_EPS)
    normed = (middle_full * row_scale * expert_norm_gain.astype(jnp.float32)).astype(jnp.bfloat16)
    shared_out = expert_apply(normed, common_gate_weight, common_up_weight, common_down_weight)
    slot_total = N_SP * CAP
    padded = jnp.concatenate([normed, jnp.zeros((1, D), normed.dtype)], axis=0)

    def one_expert(running, inputs):
        number, gate_weight, up_weight, down_weight = inputs
        matches = routes == number
        weight_row = lax.optimization_barrier(jnp.sum(jnp.where(matches, chosen_expert_weight, 0.0), axis=1))
        struck = jnp.any(matches, axis=1)
        index_rows = jnp.nonzero(struck, size=slot_total, fill_value=TOKENS)[0].astype(jnp.int32)
        answer = expert_apply(padded[index_rows], gate_weight, up_weight, down_weight).astype(jnp.bfloat16)
        weight_pad = jnp.concatenate([weight_row, jnp.zeros((1,), weight_row.dtype)], axis=0)
        running = running.at[index_rows].add(answer.astype(jnp.float32) * weight_pad[index_rows][:, None])
        return (running, None)
    routed_pad, unused = lax.scan(one_expert, jnp.zeros((TOKENS + 1, D), jnp.float32), (jnp.arange(EXPERTS, dtype=jnp.int32), routed_gate_weight, routed_up_weight, routed_down_weight))
    routed = routed_pad[:TOKENS]
    return (middle.astype(jnp.float32) + shared_out + routed).astype(jnp.bfloat16)
```

```python
import functools

import jax
import jax.numpy as jnp
from jax import lax
from jax.experimental import pallas as pl
from jax.experimental.pallas import tpu as pltpu
from jax.sharding import Mesh
from jax.sharding import PartitionSpec as P

CH = 64
CAP = 6
LANES = 128
NORM_EPS = 1e-06
GROUP_EPS = 0.00064
PLANE = ("x", "c")
SP = ("z", "x", "c")
EVERY = ("z", "x", "c", "tp")
F32 = jnp.float32
BF16 = jnp.bfloat16
NN = ((1,), (0,))
NT = ((1,), (1,))
TN = ((0,), (0,))
PAD = 104


def dot(a, b, dims=NN):
    return lax.dot_general(a, b, (dims, ((), ())), preferred_element_type=F32)


def split(a):
    high = a.astype(BF16)
    return high, (a - high.astype(F32)).astype(BF16)


def mm(a, b, dims=NN):
    ah, al = split(a)
    bh, bl = split(b)
    return dot(ah, bh, dims) + (dot(al, bh, dims) + dot(ah, bl, dims))


def iotas(rows, cols):
    return (
        lax.broadcasted_iota(jnp.int32, (rows, cols), 0),
        lax.broadcasted_iota(jnp.int32, (rows, cols), 1),
    )


def sigmoid(x):
    return 1.0 / (1.0 + jnp.exp(-x))


def unit_inverse(low):
    n = low.shape[0]
    row, col = iotas(n, n)
    size = 8
    power = jnp.where((row // size) == (col // size), low, 0.0)
    x = jnp.where(row == col, 1.0, 0.0) + power
    span = 2
    while span < size:
        power = mm(power, power)
        x = x + mm(x, power)
        span *= 2
    while size < n:
        part = ((row // (2 * size)) == (col // (2 * size))) & ((row // size) != (col // size))
        x = x + mm(mm(x, jnp.where(part, low, 0.0)), x)
        size *= 2
    return x


def mixed_of(key, learning, mix):
    return key * (1.0 + (learning - 1.0) * mix)


def routing_kernel(routes_ref, weight_ref, token_ref, slot_weight_ref):
    experts, width = token_ref.shape
    top, tokens = routes_ref.shape
    expert, token = iotas(experts, tokens)
    hit = jnp.zeros((experts, tokens), F32)
    weight = jnp.zeros((experts, tokens), F32)
    for k in range(top):
        same = routes_ref[k : k + 1, :] == expert
        hit = hit + jnp.where(same, 1.0, 0.0)
        weight = weight + jnp.where(same, weight_ref[k : k + 1, :], 0.0)
    row, col = iotas(tokens, tokens)
    earlier = jnp.where(row < col, 1.0, 0.0).astype(BF16)
    within = dot(hit.astype(BF16), earlier)
    count = jnp.sum(hit, axis=1, keepdims=True)
    slot = lax.broadcasted_iota(jnp.int32, (experts, width), 1) // (width // CAP)
    tokens_out = jnp.full((experts, width), -1.0, F32)
    weights_out = jnp.zeros((experts, width), F32)
    number = token.astype(F32)
    for m in range(CAP):
        chosen = (hit > 0.5) & (within == float(m))
        name = jnp.sum(jnp.where(chosen, number, 0.0), axis=1, keepdims=True)
        name = jnp.where(count > float(m), name, -1.0)
        part = jnp.sum(jnp.where(chosen, weight, 0.0), axis=1, keepdims=True)
        tokens_out = jnp.where(slot == m, name, tokens_out)
        weights_out = jnp.where(slot == m, part, weights_out)
    token_ref[...] = tokens_out.astype(jnp.int32)
    slot_weight_ref[...] = weights_out


def local_kernel(r_ref, k_ref, v_ref, d_ref, c_ref, mix_ref, map_ref, read_ref):
    t, w = k_ref.shape
    key = k_ref[...].astype(F32)
    learning = sigmoid(c_ref[...].astype(F32))
    log_decay = -0.6065306597126334 * sigmoid(d_ref[...].astype(F32))
    row, col = iotas(w, w)
    group = jnp.where(row // CH == col // CH, 1.0, 0.0).astype(BF16)
    square_high, square_low = split(key * key)
    length = jnp.sqrt(dot(square_high, group) + dot(square_low, group))
    unit = key / jnp.maximum(length, 1.0)
    mixed = mixed_of(key, learning, mix_ref[...])
    row, col = iotas(t, t)
    upto = jnp.where(row >= col, 1.0, 0.0).astype(BF16)
    first = log_decay.astype(BF16)
    second, third = split(log_decay - first.astype(F32))
    total = dot(upto, first) + (dot(upto, second) + dot(upto, third))
    last = total[t - 1 : t, :]
    value = v_ref[...].astype(F32)
    before = -jnp.exp(total - log_decay) * unit
    inverse_decay = jnp.exp(-total)
    rate = unit * learning
    erase = inverse_decay * rate
    write = inverse_decay * mixed
    read = jnp.exp(total) * r_ref[...].astype(F32)
    remaining = jnp.exp(last - total)
    erase_end = remaining * rate
    write_end = remaining * mixed
    final = jnp.exp(last)
    strict = row > col
    inclusive = row >= col
    hrow, hcol = iotas(CH, CH)
    for h in range(w // CH):
        s = slice(h * CH, (h + 1) * CH)
        b, q, v = before[:, s], read[:, s], value[:, s]
        pairs = mm(
            jnp.concatenate([b, q], 0), jnp.concatenate([erase[:, s], write[:, s]], 0), NT
        )
        low = jnp.where(strict, pairs[:t, :t], 0.0)
        wrote = jnp.where(strict, pairs[:t, t:], 0.0)
        read_erase = jnp.where(inclusive, pairs[t:, :t], 0.0)
        read_write = jnp.where(inclusive, pairs[t:, t:], 0.0)
        x = unit_inverse(low)
        on_values = mm(jnp.concatenate([wrote, read_write], 0), v)
        solved = mm(x, jnp.concatenate([b, on_values[:t]], 1))
        read_ref[h] = jnp.concatenate([q, on_values[t:]], 1) + mm(read_erase, solved)
        diagonal = jnp.where(hrow == hcol, jnp.broadcast_to(final[:, s], (CH, CH)), 0.0)
        state = jnp.concatenate([diagonal, mm(write_end[:, s], v, TN)], 1)
        state = state + mm(erase_end[:, s], solved, TN)
        map_ref[2 * h] = state
        map_ref[2 * h + 1] = state


def plane_kernel(map_ref, before_ref, total_ref):
    count = map_ref.shape[0]
    hrow, hcol = iotas(CH, 2 * CH)
    before_ref[0] = jnp.where(hrow == hcol, 1.0, 0.0)
    running = map_ref[0]
    for q in range(1, count):
        before_ref[q] = running
        here = map_ref[q]
        running = mm(here[:, :CH], running) + jnp.where(hcol >= CH, here, 0.0)
    for z in range(total_ref.shape[0]):
        total_ref[z] = running


def entering_kernel(place_ref, total_ref, before_ref, out_ref):
    z_here = place_ref[0]
    core = place_ref[1]
    state = jnp.zeros((CH, CH), F32)
    for z in range(total_ref.shape[0] - 1):
        here = total_ref[z]
        state = jnp.where(z < z_here, mm(here[:, :CH], state) + here[:, CH:], state)
    half = CH // 2
    start = pl.multiple_of(core * half, half)
    count = before_ref.shape[0]
    rows = jnp.concatenate([before_ref[q, pl.ds(start, half), :] for q in range(count)], 0)
    mine = mm(rows[:, :CH], state) + rows[:, CH:]
    for q in range(count):
        part = mine[q * half : (q + 1) * half]
        out_ref[q] = jnp.concatenate([part[: half // 2], part[half // 2 :]], 1)


def finish_kernel(
    state_ref, read_ref, r_ref, k_ref, v_ref, c_ref, f_ref, mix_ref, cur_ref, gain_ref, bias_ref,
    out_ref,
):
    parts = []
    for h in range(read_ref.shape[0]):
        s = slice(h * CH, (h + 1) * CH)
        even, odd = state_ref[2 * h], state_ref[2 * h + 1]
        state = jnp.concatenate([even[:, :CH], even[:, CH:], odd[:, :CH], odd[:, CH:]], 0)
        reads = read_ref[h]
        readout = reads[:, CH:] + mm(reads[:, :CH], state)
        centred = readout - jnp.mean(readout, axis=1, keepdims=True)
        spread = jnp.mean(centred * centred, axis=1, keepdims=True)
        grouped = centred * lax.rsqrt(spread + GROUP_EPS) * gain_ref[:, s] + bias_ref[:, s]
        mixed = mixed_of(
            k_ref[:, s].astype(F32), sigmoid(c_ref[:, s].astype(F32)), mix_ref[:, s]
        )
        weight = r_ref[:, s].astype(F32) * mixed * cur_ref[:, s]
        bonus = jnp.sum(weight, axis=1, keepdims=True) * v_ref[:, s].astype(F32)
        parts.append((grouped + bonus) * f_ref[:, s].astype(F32))
    out_ref[...] = jnp.concatenate(parts, 1).astype(BF16)


def project_kernel(
    place_ref, token_ref, h0_ref, h1_ref, h2_ref, h3_ref, own_ref, near_ref, far_ref, residual_ref,
    gain_ref, out_ref, normed_ref, own_middle_ref, wide_ref, rows_ref,
):
    core = place_ref[1]
    tp = place_ref[2]
    acc = dot(h0_ref[...], own_ref[...])
    half = near_ref.shape[1]
    for k, ref in enumerate((h1_ref, h2_ref, h3_ref)):
        heads = ref[...]
        low, high = heads[:, :half], heads[:, half:]
        acc = acc + dot(jnp.where(core == 0, low, high), near_ref[k])
        acc = acc + dot(jnp.where(core == 0, high, low), far_ref[k])
    middle = (residual_ref[...].astype(F32) + acc).astype(BF16)
    full = middle.astype(F32)
    scale = lax.rsqrt(jnp.mean(full * full, axis=1, keepdims=True) + NORM_EPS)
    normed = (full * scale * gain_ref[...]).astype(BF16)
    normed_ref[...] = normed
    cols = own_middle_ref.shape[1]
    own = middle[:, :cols]
    for y in range(1, middle.shape[1] // cols):
        own = jnp.where(tp == y, middle[:, y * cols : (y + 1) * cols], own)
    own_middle_ref[...] = own
    tiles = normed.shape[1] // LANES
    wide = normed.astype(F32)
    for i in range(tiles):
        wide_ref[:, i, :] = wide[:, i * LANES : (i + 1) * LANES]
    rows_ref[...] = wide_ref[...].astype(BF16)
    dests = out_ref.shape[0] // (CAP * tiles)

    def send(i, carry):
        for m in range(CAP):
            token = jnp.maximum(token_ref[((i * 4 + tp) * CAP + m) * 4], 0)
            place = pl.multiple_of((i * CAP + m) * tiles, tiles)
            out_ref[pl.ds(place, tiles), :] = rows_ref[token]
        return carry

    lax.fori_loop(0, dests, send, 0)


def shared_kernel(place_ref, normed_ref, gate_ref, up_ref, down_ref, s0_ref, s1_ref, s2_ref, s3_ref):
    tp = place_ref[2]
    gate = dot(normed_ref[...], gate_ref[...])
    up = dot(normed_ref[...], up_ref[...])
    hidden = (gate * sigmoid(gate) * up).astype(BF16)
    cols = s0_ref.shape[1]
    for k, ref in enumerate((s0_ref, s1_ref, s2_ref, s3_ref)):
        start = pl.multiple_of(lax.rem(tp + k, 4) * cols, cols)
        ref[...] = dot(hidden, down_ref[:, pl.ds(start, cols)]).astype(ref.dtype)


def expert_kernel(
    rows_ref, gate_ref, up_ref, down_ref, out_ref, wide_ref, x_ref
):
    width = gate_ref.shape[0]
    tiles = width // LANES
    block = CAP * tiles
    sources = rows_ref.shape[0] // block

    def widen(i, carry):
        wide_ref[pl.ds(pl.multiple_of(i * PAD, 8), block), :] = rows_ref[
            pl.ds(pl.multiple_of(i * block, block), block), :
        ].astype(F32)
        return carry

    lax.fori_loop(0, sources, widen, 0)
    for m in range(CAP):
        for i in range(tiles):
            x_ref[m * sources : (m + 1) * sources, i * LANES : (i + 1) * LANES] = wide_ref[
                pl.ds(m * tiles + i, sources, stride=PAD), :
            ].astype(BF16)
    x = x_ref[...]
    gate = dot(x, gate_ref[...])
    up = dot(x, up_ref[...])
    hidden = (gate * sigmoid(gate) * up).astype(BF16)
    cols = width // 4
    for y in range(4):
        answer = dot(hidden, down_ref[:, y * cols : (y + 1) * cols])
        for m in range(CAP):
            for i in range(cols // LANES):
                wide_ref[pl.ds((y * CAP + m) * (cols // LANES) + i, sources, stride=PAD), :] = answer[
                    m * sources : (m + 1) * sources, i * LANES : (i + 1) * LANES
                ]

    def narrow(i, carry):
        out_ref[pl.ds(pl.multiple_of(i * block, block), block), :] = wide_ref[
            pl.ds(pl.multiple_of(i * PAD, 8), block), :
        ].astype(BF16)
        return carry

    lax.fori_loop(0, sources, narrow, 0)


def combine_kernel(
    back_ref, token_ref, weight_ref, middle_ref, s0_ref, s1_ref, s2_ref, s3_ref, out_ref
):
    tokens, cols = out_ref.shape
    tiles = cols // LANES
    chunk = 768
    sums = [jnp.zeros((tokens, LANES), F32) for _ in range(tiles)]
    token, lane = iotas(tokens, chunk)
    for j in range(back_ref.shape[0] // chunk):
        s = slice(j * chunk, (j + 1) * chunk)
        table = jnp.where(token_ref[:, s] == token, weight_ref[:, s], 0.0)
        rows = back_ref[s, :]
        for i in range(tiles):
            part = jnp.where(lane % tiles == i, table, 0.0).astype(BF16)
            sums[i] = sums[i] + dot(part, rows)
    total = middle_ref[...].astype(F32) + s0_ref[...] + s1_ref[...].astype(F32)
    total = total + s2_ref[...].astype(F32) + s3_ref[...].astype(F32)
    out_ref[...] = (total + jnp.concatenate(sums, 1)).astype(BF16)


def call(kernel, name, out, *args, scalars=0, scratch=()):
    smem = pl.BlockSpec(memory_space=pltpu.SMEM)
    vmem = pl.BlockSpec(memory_space=pltpu.VMEM)
    return pl.pallas_call(
        kernel,
        out_shape=out,
        in_specs=[smem] * scalars + [vmem] * (len(args) - scalars),
        out_specs=jax.tree.map(lambda _: vmem, out),
        scratch_shapes=list(scratch),
        name=name,
    )(*args)


def exchange(array, axes):
    return lax.all_to_all(array, axes, split_axis=0, concat_axis=0, tiled=True)


def turned(array, axis, shift):
    peers = lax.axis_size(axis)
    return lax.ppermute(array, axis, [(i, (i + shift) % peers) for i in range(peers)])


def per_device(
    receptance, key, value, decay, correction, factor, mix, current, gain, bias, output_matrix,
    residual, norm_gain, routes, chosen, routed_gate, routed_up, routed_down, common_gate,
    common_up, common_down,
):
    shape = jax.ShapeDtypeStruct
    tokens, inner = key.shape
    width = residual.shape[1]
    cols = width // 4
    heads = inner // CH
    z_count, plane = lax.axis_size("z"), lax.axis_size(PLANE)
    experts = lax.axis_size(EVERY)
    slots = lax.axis_size(SP) * CAP
    core = lax.axis_index("c")
    place = jnp.stack([lax.axis_index("z"), core, lax.axis_index("tp")]).astype(jnp.int32)
    mix, current, gain, bias = (a.reshape(1, -1) for a in (mix, current, gain, bias))

    half = inner // 2
    mine = lax.dynamic_slice_in_dim(output_matrix, core * half, half, 0)
    near = jnp.stack([turned(mine, "tp", k) for k in (1, 2, 3)])
    far = turned(near, "c", 1)

    table = (shape((experts, CAP * 4), jnp.int32), shape((experts, CAP * 4), F32))
    slot_token, slot_weight = call(routing_kernel, "routing", table, routes.T, chosen.T)
    slot_token = slot_token.reshape(-1)
    slot_weight = slot_weight.reshape(1, -1)

    maps, reads = call(
        local_kernel, "local_terms",
        (shape((2 * heads, CH, 2 * CH), F32), shape((heads, tokens, 2 * CH), F32)),
        receptance, key, value, decay, correction, mix,
    )
    maps = exchange(maps, PLANE)
    before, totals = call(
        plane_kernel, "plane_prefix",
        (shape((plane, CH, 2 * CH), F32), shape((z_count, CH, 2 * CH), F32)), maps,
    )
    totals = exchange(totals, "z")
    states = call(
        entering_kernel, "entering", shape((plane, CH // 4, 2 * CH), F32), place, totals, before,
        scalars=1,
    )
    states = exchange(states, PLANE)
    mixed = call(
        finish_kernel, "finish", shape((tokens, inner), BF16), states, reads, receptance, key,
        value, correction, factor, mix, current, gain, bias,
    )
    others = [turned(mixed, "tp", k) for k in (1, 2, 3)]
    outgoing, normed, own_middle = call(
        project_kernel, "project",
        (
            shape((slots * width // LANES, LANES), BF16),
            shape((tokens, width), BF16),
            shape((tokens, cols), BF16),
        ),
        place, slot_token, mixed, *others, output_matrix, near, far, residual,
        norm_gain.reshape(1, -1),
        scalars=2,
        scratch=(
            pltpu.VMEM((tokens, width // LANES, LANES), F32),
            pltpu.VMEM((tokens, width // LANES, LANES), BF16),
        ),
    )
    arrived = exchange(outgoing, SP)
    shared = call(
        shared_kernel, "shared",
        (shape((tokens, cols), F32),) + (shape((tokens, cols), BF16),) * 3,
        place, normed, common_gate, common_up, common_down, scalars=1,
    )
    shared = [shared[0]] + [turned(shared[k], "tp", k) for k in (1, 2, 3)]
    answer = call(
        expert_kernel, "expert", shape(outgoing.shape, BF16), arrived, routed_gate[0],
        routed_up[0], routed_down[0],
        scratch=(
            pltpu.VMEM((slots // CAP * PAD, LANES), F32),
            pltpu.VMEM((slots, width), BF16),
        ),
    )
    back = exchange(answer, EVERY)
    return call(
        combine_kernel, "combine", shape((tokens, cols), BF16), back, slot_token.reshape(1, -1),
        slot_weight, own_middle, *shared,
    )


def solution(mesh):
    finer = Mesh(mesh.devices.reshape(8, 4, 2, mesh.shape["tp"]), EVERY)
    placed = (
        (P(SP, "tp"),) * 6
        + (P("tp"),) * 4
        + (P("tp", None), P(SP, None), P(), P(SP, None), P(SP, None))
        + (P(EVERY, None, None),) * 3
        + (P(None, "tp"), P(None, "tp"), P("tp", None))
    )
    return jax.shard_map(
        per_device, mesh=finer, in_specs=placed, out_specs=P(SP, "tp"), check_vma=False
    )
```

```python
import functools

import jax
import jax.numpy as jnp
from jax import lax
from jax.experimental import pallas as pl
from jax.experimental.pallas import tpu as pltpu
from jax.sharding import Mesh
from jax.sharding import PartitionSpec as P

CH = 64
CAP = 6
LANES = 128
NORM_EPS = 1e-06
GROUP_EPS = 0.00064
PLANE = ("x", "c")
SP = ("z", "x", "c")
EVERY = ("z", "x", "c", "tp")
F32 = jnp.float32
BF16 = jnp.bfloat16
NN = ((1,), (0,))
NT = ((1,), (1,))
TN = ((0,), (0,))
PAD = 104


def dot(a, b, dims=NN):
    return lax.dot_general(a, b, (dims, ((), ())), preferred_element_type=F32)


def split(a):
    high = a.astype(BF16)
    return high, (a - high.astype(F32)).astype(BF16)


def mm(a, b, dims=NN):
    ah, al = split(a)
    bh, bl = split(b)
    return dot(ah, bh, dims) + (dot(al, bh, dims) + dot(ah, bl, dims))


def iotas(rows, cols):
    return (
        lax.broadcasted_iota(jnp.int32, (rows, cols), 0),
        lax.broadcasted_iota(jnp.int32, (rows, cols), 1),
    )


def sigmoid(x):
    return 1.0 / (1.0 + jnp.exp(-x))


def unit_inverses(lows):
    n = lows[0].shape[0]
    row, col = iotas(n, n)
    size = 8
    eye = jnp.where(row == col, 1.0, 0.0)
    inside = (row // size) == (col // size)
    powers = [jnp.where(inside, low, 0.0) for low in lows]
    xs = [eye + power for power in powers]
    span = 2
    while span < size:
        powers = [mm(power, power) for power in powers]
        xs = [x + mm(x, power) for x, power in zip(xs, powers)]
        span *= 2
    while size < n:
        part = ((row // (2 * size)) == (col // (2 * size))) & ((row // size) != (col // size))
        lefts = [mm(x, jnp.where(part, low, 0.0)) for x, low in zip(xs, lows)]
        xs = [x + mm(left, x) for x, left in zip(xs, lefts)]
        size *= 2
    return xs


def mixed_of(key, learning, mix):
    return key * (1.0 + (learning - 1.0) * mix)


def routing_kernel(routes_ref, weight_ref, token_ref, slot_weight_ref):
    experts, width = token_ref.shape
    top, tokens = routes_ref.shape
    expert, token = iotas(experts, tokens)
    hit = jnp.zeros((experts, tokens), F32)
    weight = jnp.zeros((experts, tokens), F32)
    for k in range(top):
        same = routes_ref[k : k + 1, :] == expert
        hit = hit + jnp.where(same, 1.0, 0.0)
        weight = weight + jnp.where(same, weight_ref[k : k + 1, :], 0.0)
    row, col = iotas(tokens, tokens)
    earlier = jnp.where(row < col, 1.0, 0.0).astype(BF16)
    within = dot(hit.astype(BF16), earlier)
    count = jnp.sum(hit, axis=1, keepdims=True)
    slot = lax.broadcasted_iota(jnp.int32, (experts, width), 1) // (width // CAP)
    tokens_out = jnp.full((experts, width), -1.0, F32)
    weights_out = jnp.zeros((experts, width), F32)
    number = token.astype(F32)
    for m in range(CAP):
        chosen = (hit > 0.5) & (within == float(m))
        name = jnp.sum(jnp.where(chosen, number, 0.0), axis=1, keepdims=True)
        name = jnp.where(count > float(m), name, -1.0)
        part = jnp.sum(jnp.where(chosen, weight, 0.0), axis=1, keepdims=True)
        tokens_out = jnp.where(slot == m, name, tokens_out)
        weights_out = jnp.where(slot == m, part, weights_out)
    token_ref[...] = tokens_out.astype(jnp.int32)
    slot_weight_ref[...] = weights_out


def local_kernel(r_ref, k_ref, v_ref, d_ref, c_ref, mix_ref, map_ref, read_ref):
    t, w = k_ref.shape
    key = k_ref[...].astype(F32)
    learning = sigmoid(c_ref[...].astype(F32))
    log_decay = -0.6065306597126334 * sigmoid(d_ref[...].astype(F32))
    row, col = iotas(w, w)
    group = jnp.where(row // CH == col // CH, 1.0, 0.0).astype(BF16)
    square_high, square_low = split(key * key)
    length = jnp.sqrt(dot(square_high, group) + dot(square_low, group))
    unit = key / jnp.maximum(length, 1.0)
    mixed = mixed_of(key, learning, mix_ref[...])
    row, col = iotas(t, t)
    upto = jnp.where(row >= col, 1.0, 0.0).astype(BF16)
    first = log_decay.astype(BF16)
    second, third = split(log_decay - first.astype(F32))
    total = dot(upto, first) + (dot(upto, second) + dot(upto, third))
    last = total[t - 1 : t, :]
    value = v_ref[...].astype(F32)
    before = -jnp.exp(total - log_decay) * unit
    inverse_decay = jnp.exp(-total)
    rate = unit * learning
    erase = inverse_decay * rate
    write = inverse_decay * mixed
    read = jnp.exp(total) * r_ref[...].astype(F32)
    remaining = jnp.exp(last - total)
    erase_end = remaining * rate
    write_end = remaining * mixed
    final = jnp.exp(last)
    strict = row > col
    inclusive = row >= col
    hrow, hcol = iotas(CH, CH)
    every = range(w // CH)

    def parts(array):
        return [array[:, h * CH : (h + 1) * CH] for h in every]

    befores, asked, values = parts(before), parts(read), parts(value)
    pairs = [
        mm(jnp.concatenate([b, q], 0), jnp.concatenate([e, x], 0), NT)
        for b, q, e, x in zip(befores, asked, parts(erase), parts(write))
    ]
    lows = [jnp.where(strict, p[:t, :t], 0.0) for p in pairs]
    stacks = [
        jnp.concatenate(
            [jnp.where(strict, p[:t, t:], 0.0), jnp.where(inclusive, p[t:, t:], 0.0)], 0
        )
        for p in pairs
    ]
    on_values = [mm(stack, v) for stack, v in zip(stacks, values)]
    written = [mm(e, v, TN) for e, v in zip(parts(write_end), values)]
    xs = unit_inverses(lows)
    solved = [
        mm(x, jnp.concatenate([b, o[:t]], 1)) for x, b, o in zip(xs, befores, on_values)
    ]
    states = [mm(e, z, TN) for e, z in zip(parts(erase_end), solved)]
    reads = [mm(jnp.where(inclusive, p[t:, :t], 0.0), z) for p, z in zip(pairs, solved)]
    for h, f in zip(every, parts(final)):
        diagonal = jnp.where(hrow == hcol, jnp.broadcast_to(f, (CH, CH)), 0.0)
        state = states[h] + jnp.concatenate([diagonal, written[h]], 1)
        map_ref[2 * h] = state
        map_ref[2 * h + 1] = state
        read_ref[h] = reads[h] + jnp.concatenate([asked[h], on_values[h][t:]], 1)


def joined(former, latter, late):
    return mm(latter[:, :CH], former) + jnp.where(late, latter, 0.0)


def plane_kernel(map_ref, before_ref, total_ref):
    count = map_ref.shape[0]
    hrow, hcol = iotas(CH, 2 * CH)
    late = hcol >= CH
    maps = [map_ref[q] for q in range(count)]
    span = 1
    while span < count:
        maps = [
            maps[q] if q < span else joined(maps[q - span], maps[q], late) for q in range(count)
        ]
        span *= 2
    before_ref[0] = jnp.where(hrow == hcol, 1.0, 0.0)
    for q in range(1, count):
        before_ref[q] = maps[q - 1]
    total_ref[...] = maps[count - 1]


def entering_kernel(place_ref, before_ref, *refs):
    *earlier_refs, out_ref = refs
    z_here = place_ref[0]
    core = place_ref[1]
    hrow, hcol = iotas(CH, 2 * CH)
    late = hcol >= CH
    nothing = jnp.where(hrow == hcol, 1.0, 0.0)
    maps = [
        jnp.where(z_here >= k, earlier_refs[k - 1][...], nothing)
        for k in range(len(earlier_refs), 0, -1)
    ]
    while len(maps) > 1:
        odd = maps[:1] if len(maps) % 2 else []
        rest = maps[len(odd) :]
        maps = odd + [
            joined(rest[i], rest[i + 1], late) for i in range(0, len(rest), 2)
        ]
    state = maps[0][:, CH:]
    half = CH // 2
    start = pl.multiple_of(core * half, half)
    count = before_ref.shape[0]
    rows = jnp.concatenate([before_ref[q, pl.ds(start, half), :] for q in range(count)], 0)
    mine = mm(rows[:, :CH], state) + rows[:, CH:]
    for q in range(count):
        part = mine[q * half : (q + 1) * half]
        out_ref[q] = jnp.concatenate([part[: half // 2], part[half // 2 :]], 1)


def finish_kernel(
    state_ref, read_ref, r_ref, k_ref, v_ref, c_ref, f_ref, mix_ref, cur_ref, gain_ref, bias_ref,
    out_ref,
):
    every = range(read_ref.shape[0])
    slices = [slice(h * CH, (h + 1) * CH) for h in every]
    mixed = mixed_of(k_ref[...].astype(F32), sigmoid(c_ref[...].astype(F32)), mix_ref[...])
    weight = r_ref[...].astype(F32) * mixed * cur_ref[...]
    readouts = []
    for h in every:
        even, odd = state_ref[2 * h], state_ref[2 * h + 1]
        state = jnp.concatenate([even[:, :CH], even[:, CH:], odd[:, :CH], odd[:, CH:]], 0)
        reads = read_ref[h]
        readouts.append(reads[:, CH:] + mm(reads[:, :CH], state))
    bonuses = [jnp.sum(weight[:, s], axis=1, keepdims=True) for s in slices]
    means = [jnp.mean(readout, axis=1, keepdims=True) for readout in readouts]
    centred = [readout - mean for readout, mean in zip(readouts, means)]
    spreads = [jnp.mean(c * c, axis=1, keepdims=True) for c in centred]
    scaled = [c * lax.rsqrt(spread + GROUP_EPS) for c, spread in zip(centred, spreads)]
    wide = (readouts[0].shape[0], CH)
    bonus = jnp.concatenate([jnp.broadcast_to(b, wide) for b in bonuses], 1)
    grouped = jnp.concatenate(scaled, 1) * gain_ref[...] + bias_ref[...]
    out = (grouped + bonus * v_ref[...].astype(F32)) * f_ref[...].astype(F32)
    out_ref[...] = out.astype(BF16)


def fetch(sources, targets, sems):
    copies = [
        pltpu.make_async_copy(source, target, sems.at[i])
        for i, (source, target) in enumerate(zip(sources, targets))
    ]
    for copy in copies:
        copy.start()
    return copies


def project_kernel(
    place_ref, token_ref, h0_ref, h1_ref, h2_ref, h3_ref, gain_ref, own_hbm, near_hbm, far_hbm,
    residual_hbm, out_ref, normed_ref, own_middle_ref, own_ref, near_ref, far_ref, residual_ref,
    wide_ref, rows_ref, sems,
):
    core = place_ref[1]
    tp = place_ref[2]
    copies = fetch(
        (own_hbm, near_hbm, far_hbm, residual_hbm), (own_ref, near_ref, far_ref, residual_ref), sems
    )
    copies[0].wait()
    acc = dot(h0_ref[...], own_ref[...])
    half = near_ref.shape[1]
    heads = [ref[...] for ref in (h1_ref, h2_ref, h3_ref)]
    copies[1].wait()
    for k, head in enumerate(heads):
        acc = acc + dot(jnp.where(core == 0, head[:, :half], head[:, half:]), near_ref[k])
    copies[2].wait()
    for k, head in enumerate(heads):
        acc = acc + dot(jnp.where(core == 0, head[:, half:], head[:, :half]), far_ref[k])
    copies[3].wait()
    middle = (residual_ref[...].astype(F32) + acc).astype(BF16)
    full = middle.astype(F32)
    scale = lax.rsqrt(jnp.mean(full * full, axis=1, keepdims=True) + NORM_EPS)
    normed = (full * scale * gain_ref[...]).astype(BF16)
    normed_ref[...] = normed
    cols = own_middle_ref.shape[1]
    own = middle[:, :cols]
    for y in range(1, middle.shape[1] // cols):
        own = jnp.where(tp == y, middle[:, y * cols : (y + 1) * cols], own)
    own_middle_ref[...] = own
    tiles = normed.shape[1] // LANES
    wide = normed.astype(F32)
    for i in range(tiles):
        wide_ref[:, i, :] = wide[:, i * LANES : (i + 1) * LANES]
    rows_ref[...] = wide_ref[:, :tiles, :].astype(BF16)
    dests = out_ref.shape[0] // (CAP * tiles)

    def send(i, carry):
        for m in range(CAP):
            token = jnp.maximum(token_ref[(i * 4 + tp) * CAP + m], 0)
            place = pl.multiple_of((i * CAP + m) * tiles, tiles)
            out_ref[pl.ds(place, tiles), :] = rows_ref[token]
        return carry

    lax.fori_loop(0, dests, send, 0, unroll=4)


def shared_kernel(place_ref, normed_ref, gate_ref, up_ref, down_ref, s0_ref, s1_ref, s2_ref, s3_ref):
    tp = place_ref[2]
    gate = dot(normed_ref[...], gate_ref[...])
    up = dot(normed_ref[...], up_ref[...])
    hidden = (gate * sigmoid(gate) * up).astype(BF16)
    cols = s0_ref.shape[1]
    for k, ref in enumerate((s0_ref, s1_ref, s2_ref, s3_ref)):
        start = pl.multiple_of(lax.rem(tp + k, 4) * cols, cols)
        ref[...] = dot(hidden, down_ref[:, pl.ds(start, cols)]).astype(ref.dtype)


def expert_kernel(
    rows_ref, gate_hbm, up_hbm, down_hbm, out_ref, gate_ref, up_ref, down_ref, wide_ref, x_ref, sems
):
    copies = fetch((gate_hbm, up_hbm, down_hbm), (gate_ref, up_ref, down_ref), sems)
    width = gate_ref.shape[0]
    tiles = width // LANES
    block = CAP * tiles
    sources = rows_ref.shape[0] // block

    def widen(i, carry):
        wide_ref[pl.ds(pl.multiple_of(i * PAD, 8), block), :] = rows_ref[
            pl.ds(pl.multiple_of(i * block, block), block), :
        ].astype(F32)
        return carry

    lax.fori_loop(0, sources, widen, 0, unroll=4)
    for m in range(CAP):
        for i in range(tiles):
            x_ref[m * sources : (m + 1) * sources, i * LANES : (i + 1) * LANES] = wide_ref[
                pl.ds(m * tiles + i, sources, stride=PAD), :
            ].astype(BF16)
    x = x_ref[...]
    copies[0].wait()
    gate = dot(x, gate_ref[...])
    copies[1].wait()
    up = dot(x, up_ref[...])
    hidden = (gate * sigmoid(gate) * up).astype(BF16)
    cols = width // 4
    copies[2].wait()
    for y in range(4):
        answer = dot(hidden, down_ref[:, y * cols : (y + 1) * cols])
        for m in range(CAP):
            for i in range(cols // LANES):
                place = (y * CAP + m) * (cols // LANES) + i
                wide_ref[pl.ds(place, sources, stride=PAD), :] = answer[
                    m * sources : (m + 1) * sources, i * LANES : (i + 1) * LANES
                ]

    def narrow(i, carry):
        out_ref[pl.ds(pl.multiple_of(i * block, block), block), :] = wide_ref[
            pl.ds(pl.multiple_of(i * PAD, 8), block), :
        ].astype(BF16)
        return carry

    lax.fori_loop(0, sources, narrow, 0, unroll=4)


def combine_kernel(
    back_ref, token_ref, weight_ref, middle_ref, s0_ref, s1_ref, s2_ref, s3_ref, out_ref, wide_ref
):
    tokens, cols = out_ref.shape
    tiles = cols // LANES
    slots = back_ref.shape[0] // tiles
    wide_ref[...] = back_ref[...].astype(F32)
    token, _ = iotas(tokens, slots)
    table = jnp.where(token_ref[...] == token, weight_ref[...], 0.0).astype(BF16)
    rows = jnp.concatenate(
        [wide_ref[pl.ds(i, slots, stride=tiles), :].astype(BF16) for i in range(tiles)], 1
    )
    total = middle_ref[...].astype(F32) + s0_ref[...] + s1_ref[...].astype(F32)
    total = total + s2_ref[...].astype(F32) + s3_ref[...].astype(F32)
    out_ref[...] = (total + dot(table, rows)).astype(BF16)


def call(kernel, name, out, *args, scalars=0, fetched=0, scratch=()):
    smem = pl.BlockSpec(memory_space=pltpu.SMEM)
    vmem = pl.BlockSpec(memory_space=pltpu.VMEM)
    hbm = pl.BlockSpec(memory_space=pl.ANY)
    loaded = len(args) - scalars - fetched
    scratch = list(scratch)
    if fetched:
        scratch = [pltpu.VMEM(a.shape, a.dtype) for a in args[-fetched:]] + scratch
        scratch.append(pltpu.SemaphoreType.DMA((fetched,)))
    return pl.pallas_call(
        kernel,
        out_shape=out,
        in_specs=[smem] * scalars + [vmem] * loaded + [hbm] * fetched,
        out_specs=jax.tree.map(lambda _: vmem, out),
        scratch_shapes=scratch,
        name=name,
    )(*args)


def exchange(array, axes):
    return lax.all_to_all(array, axes, split_axis=0, concat_axis=0, tiled=True)


def turned(array, axis, shift):
    peers = lax.axis_size(axis)
    return lax.ppermute(array, axis, [(i, (i + shift) % peers) for i in range(peers)])


def per_device(
    receptance, key, value, decay, correction, factor, mix, current, gain, bias, output_matrix,
    residual, norm_gain, routes, chosen, routed_gate, routed_up, routed_down, common_gate,
    common_up, common_down,
):
    shape = jax.ShapeDtypeStruct
    tokens, inner = key.shape
    width = residual.shape[1]
    cols = width // 4
    heads = inner // CH
    z_count, plane = lax.axis_size("z"), lax.axis_size(PLANE)
    experts = lax.axis_size(EVERY)
    slots = lax.axis_size(SP) * CAP
    core = lax.axis_index("c")
    place = jnp.stack([lax.axis_index("z"), core, lax.axis_index("tp")]).astype(jnp.int32)
    mix, current, gain, bias = (a.reshape(1, -1) for a in (mix, current, gain, bias))

    half = inner // 2
    mine = lax.dynamic_slice_in_dim(output_matrix, core * half, half, 0)
    near = [turned(mine, "tp", k) for k in (1, 2, 3)]

    table = (shape((experts, CAP), jnp.int32), shape((experts, CAP), F32))
    slot_token, slot_weight = call(routing_kernel, "routing", table, routes.T, chosen.T)
    slot_token = slot_token.reshape(-1)
    slot_weight = slot_weight.reshape(1, -1)

    maps, reads = call(
        local_kernel, "local_terms",
        (shape((2 * heads, CH, 2 * CH), F32), shape((heads, tokens, 2 * CH), F32)),
        receptance, key, value, decay, correction, mix,
    )
    maps = exchange(maps, PLANE)
    before, total = call(
        plane_kernel, "plane_prefix",
        (shape((plane, CH, 2 * CH), F32), shape((CH, 2 * CH), F32)), maps,
    )
    earlier = [turned(total, "z", k) for k in range(1, z_count)]
    states = call(
        entering_kernel, "entering", shape((plane, CH // 4, 2 * CH), F32), place, before, *earlier,
        scalars=1,
    )
    states, *near = lax.optimization_barrier((states, *near))
    near = jnp.stack(near)
    far = turned(near, "c", 1)
    states = exchange(states, PLANE)
    mixed = call(
        finish_kernel, "finish", shape((tokens, inner), BF16), states, reads, receptance, key,
        value, correction, factor, mix, current, gain, bias,
    )
    others = [turned(mixed, "tp", k) for k in (1, 2, 3)]
    outgoing, normed, own_middle = call(
        project_kernel, "project",
        (
            shape((slots * width // LANES, LANES), BF16),
            shape((tokens, width), BF16),
            shape((tokens, cols), BF16),
        ),
        place, slot_token, mixed, *others, norm_gain.reshape(1, -1), output_matrix, near, far,
        residual,
        scalars=2,
        fetched=4,
        scratch=(
            pltpu.VMEM((tokens, width // LANES + 8, LANES), F32),
            pltpu.VMEM((tokens, width // LANES, LANES), BF16),
        ),
    )
    arrived = exchange(outgoing, SP)
    shared = call(
        shared_kernel, "shared",
        (shape((tokens, cols), F32),) + (shape((tokens, cols), BF16),) * 3,
        place, normed, common_gate, common_up, common_down, scalars=1,
    )
    shared = [shared[0]] + [turned(shared[k], "tp", k) for k in (1, 2, 3)]
    answer = call(
        expert_kernel, "expert", shape(outgoing.shape, BF16), arrived, routed_gate[0],
        routed_up[0], routed_down[0],
        fetched=3,
        scratch=(
            pltpu.VMEM((slots // CAP * PAD, LANES), F32),
            pltpu.VMEM((slots, width), BF16),
        ),
    )
    back = exchange(answer, EVERY)
    return call(
        combine_kernel, "combine", shape((tokens, cols), BF16), back, slot_token.reshape(1, -1),
        slot_weight, own_middle, *shared,
        scratch=(pltpu.VMEM(back.shape, F32),),
    )


def solution(mesh):
    finer = Mesh(mesh.devices.reshape(8, 4, 2, mesh.shape["tp"]), EVERY)
    placed = (
        (P(SP, "tp"),) * 6
        + (P("tp"),) * 4
        + (P("tp", None), P(SP, None), P(), P(SP, None), P(SP, None))
        + (P(EVERY, None, None),) * 3
        + (P(None, "tp"), P(None, "tp"), P("tp", None))
    )
    return jax.shard_map(
        per_device, mesh=finer, in_specs=placed, out_specs=P(SP, "tp"), check_vma=False
    )
```

```python
import jax
import jax.numpy as jnp
from jax import lax
from jax.experimental import pallas as pl
from jax.experimental.pallas import tpu as pltpu
from jax.sharding import Mesh
from jax.sharding import PartitionSpec as P


CH = 64
CAP = 6
LANES = 128
NORM_EPS = 1e-06
GROUP_EPS = 0.00064
PLANE = ("x", "c")
SP = ("z", "x", "c")
EVERY = ("z", "x", "c", "tp")
F32 = jnp.float32
BF16 = jnp.bfloat16
NN = ((1,), (0,))
NT = ((1,), (1,))
TN = ((0,), (0,))
PAD = 104


def dot(a, b, dims=NN):
    return lax.dot_general(a, b, (dims, ((), ())), preferred_element_type=F32)


def split(a):
    high = a.astype(BF16)
    return high, (a - high.astype(F32)).astype(BF16)


def mm(a, b, dims=NN):
    ah, al = split(a)
    bh, bl = split(b)
    return dot(ah, bh, dims) + (dot(al, bh, dims) + dot(ah, bl, dims))


def iotas(rows, cols):
    return (
        lax.broadcasted_iota(jnp.int32, (rows, cols), 0),
        lax.broadcasted_iota(jnp.int32, (rows, cols), 1),
    )


def sigmoid(x):
    return 1.0 / (1.0 + jnp.exp(-x))


def unit_inverses(lows):
    n = lows[0].shape[0]
    row, col = iotas(n, n)
    size = 8
    eye = jnp.where(row == col, 1.0, 0.0)
    inside = (row // size) == (col // size)
    powers = [jnp.where(inside, low, 0.0) for low in lows]
    xs = [eye + power for power in powers]
    span = 2
    while span < size:
        powers = [mm(power, power) for power in powers]
        xs = [x + mm(x, power) for x, power in zip(xs, powers)]
        span *= 2
    while size < n:
        part = ((row // (2 * size)) == (col // (2 * size))) & ((row // size) != (col // size))
        lefts = [mm(x, jnp.where(part, low, 0.0)) for x, low in zip(xs, lows)]
        xs = [x + mm(left, x) for x, left in zip(xs, lefts)]
        size *= 2
    return xs


def mixed_of(key, learning, mix):
    return key * (1.0 + (learning - 1.0) * mix)


def routing_kernel(routes_ref, weight_ref, token_ref, slot_weight_ref):
    slots, experts = token_ref.shape
    tokens, top = routes_ref.shape
    token, expert = iotas(tokens, experts)
    weight = jnp.zeros((tokens, experts), F32)
    hit = jnp.zeros((tokens, experts), F32)
    for k in range(top):
        same = routes_ref[:, k : k + 1] == expert
        hit = jnp.where(same, 1.0, hit)
        weight = jnp.where(same, weight_ref[:, k : k + 1], weight)
    row, col = iotas(tokens, tokens)
    earlier = jnp.where(row > col, 1.0, 0.0).astype(BF16)
    within = dot(earlier, hit.astype(BF16))
    within = jnp.where(hit > 0.5, within, -1.0)
    number = token.astype(F32) + 1.0
    for m in range(slots):
        chosen = within == float(m)
        name = jnp.sum(jnp.where(chosen, number, 0.0), axis=0, keepdims=True) - 1.0
        token_ref[m : m + 1, :] = name.astype(jnp.int32)
        slot_weight_ref[m : m + 1, :] = jnp.sum(
            jnp.where(chosen, weight, 0.0), axis=0, keepdims=True
        )


def local_kernel(r_ref, k_ref, v_ref, d_ref, c_ref, mix_ref, map_ref, read_ref):
    t, w = k_ref.shape
    key = k_ref[...].astype(F32)
    learning = sigmoid(c_ref[...].astype(F32))
    log_decay = -0.6065306597126334 * sigmoid(d_ref[...].astype(F32))
    row, col = iotas(w, w)
    group = jnp.where(row // CH == col // CH, 1.0, 0.0).astype(BF16)
    square_high, square_low = split(key * key)
    length = jnp.sqrt(dot(square_high, group) + dot(square_low, group))
    unit = key / jnp.maximum(length, 1.0)
    mixed = mixed_of(key, learning, mix_ref[...])
    row, col = iotas(t, t)
    upto = jnp.where(row >= col, 1.0, 0.0).astype(BF16)
    first = log_decay.astype(BF16)
    second, third = split(log_decay - first.astype(F32))
    total = dot(upto, first) + (dot(upto, second) + dot(upto, third))
    last = total[t - 1 : t, :]
    value = v_ref[...].astype(F32)
    before = -jnp.exp(total - log_decay) * unit
    inverse_decay = jnp.exp(-total)
    rate = unit * learning
    erase = inverse_decay * rate
    write = inverse_decay * mixed
    read = jnp.exp(total) * r_ref[...].astype(F32)
    remaining = jnp.exp(last - total)
    erase_end = remaining * rate
    write_end = remaining * mixed
    final = jnp.exp(last)
    strict = row > col
    inclusive = row >= col
    hrow, hcol = iotas(CH, CH)
    every = range(w // CH)

    def parts(array):
        return [array[:, h * CH : (h + 1) * CH] for h in every]

    befores, asked, values = parts(before), parts(read), parts(value)
    pairs = [
        mm(jnp.concatenate([b, q], 0), jnp.concatenate([e, x], 0), NT)
        for b, q, e, x in zip(befores, asked, parts(erase), parts(write))
    ]
    lows = [jnp.where(strict, p[:t, :t], 0.0) for p in pairs]
    stacks = [
        jnp.concatenate(
            [jnp.where(strict, p[:t, t:], 0.0), jnp.where(inclusive, p[t:, t:], 0.0)], 0
        )
        for p in pairs
    ]
    on_values = [mm(stack, v) for stack, v in zip(stacks, values)]
    written = [mm(e, v, TN) for e, v in zip(parts(write_end), values)]
    xs = unit_inverses(lows)
    solved = [
        mm(x, jnp.concatenate([b, o[:t]], 1)) for x, b, o in zip(xs, befores, on_values)
    ]
    states = [mm(e, z, TN) for e, z in zip(parts(erase_end), solved)]
    reads = [mm(jnp.where(inclusive, p[t:, :t], 0.0), z) for p, z in zip(pairs, solved)]
    for h, f in zip(every, parts(final)):
        diagonal = jnp.where(hrow == hcol, jnp.broadcast_to(f, (CH, CH)), 0.0)
        state = states[h] + jnp.concatenate([diagonal, written[h]], 1)
        map_ref[2 * h], map_ref[2 * h + 1] = packed(state)
        read_ref[h] = reads[h] + jnp.concatenate([asked[h], on_values[h][t:]], 1)


def packed(state):
    half = CH // 2
    left = jnp.concatenate([state[:half, :CH], state[half:, :CH]], 1)
    quarter = half // 2
    pieces = []
    for c in range(2):
        cols = state[:, CH + c * half : CH + (c + 1) * half]
        rows = [cols[i * quarter : (i + 1) * quarter] for i in range(4)]
        pieces.append(jnp.concatenate([left, jnp.concatenate(rows, 1)], 0))
    return pieces


def repacked(state):
    half = CH // 2
    quarter = half // 2
    left = jnp.concatenate([state[:half, :CH], state[half:, :CH]], 1)
    rows = [state[i * quarter : (i + 1) * quarter, CH:] for i in range(4)]
    return jnp.concatenate([left, jnp.concatenate(rows, 1)], 0)


def unpacked(block):
    half = CH // 2
    left = jnp.concatenate([block[:half, :CH], block[:half, CH:]], 0)
    right = jnp.concatenate([block[half:, i * half : (i + 1) * half] for i in range(4)], 0)
    return jnp.concatenate([left, right], 1)


def joined(former, latter, late):
    return mm(latter[:, :CH], former) + jnp.where(late, latter, 0.0)


def plane_kernel(map_ref, before_ref, total_ref):
    count = map_ref.shape[0]
    hrow, hcol = iotas(CH, 3 * CH // 2)
    late = hcol >= CH
    maps = [unpacked(map_ref[q]) for q in range(count)]
    span = 1
    while span < count:
        maps = [
            maps[q] if q < span else joined(maps[q - span], maps[q], late) for q in range(count)
        ]
        span *= 2
    total = repacked(maps[count - 1])
    for z in range(total_ref.shape[0]):
        total_ref[z] = total
    before_ref[0] = jnp.where(hrow == hcol, 1.0, 0.0)
    for q in range(1, count):
        before_ref[q] = maps[q - 1]


def entering_kernel(place_ref, before_ref, total_ref, out_ref):
    z_here = place_ref[0]
    hrow, hcol = iotas(CH, 3 * CH // 2)
    late = hcol >= CH
    nothing = jnp.where(hrow == hcol, 1.0, 0.0)
    maps = [
        jnp.where(z < z_here, unpacked(total_ref[z]), nothing)
        for z in range(total_ref.shape[0] - 1)
    ]
    while len(maps) > 1:
        odd = maps[:1] if len(maps) % 2 else []
        rest = maps[len(odd) :]
        maps = odd + [
            joined(rest[i], rest[i + 1], late) for i in range(0, len(rest), 2)
        ]
    state = maps[0][:, CH:]
    count = before_ref.shape[0]
    rows = jnp.concatenate([before_ref[q] for q in range(count)], 0)
    mine = mm(rows[:, :CH], state) + rows[:, CH:]
    quarter = CH // 4
    for q in range(count):
        pieces = [mine[q * CH + i * quarter : q * CH + (i + 1) * quarter] for i in range(4)]
        out_ref[q] = jnp.concatenate(pieces, 1)


def finish_kernel(
    state_ref, read_ref, r_ref, k_ref, v_ref, c_ref, f_ref, mix_ref, cur_ref, gain_ref, bias_ref,
    out_ref,
):
    every = range(read_ref.shape[0])
    slices = [slice(h * CH, (h + 1) * CH) for h in every]
    mixed = mixed_of(k_ref[...].astype(F32), sigmoid(c_ref[...].astype(F32)), mix_ref[...])
    weight = r_ref[...].astype(F32) * mixed * cur_ref[...]
    readouts = []
    for h in every:
        even, odd = state_ref[2 * h], state_ref[2 * h + 1]
        half = CH // 2
        state = jnp.concatenate(
            [
                jnp.concatenate([ref[:, i * half : (i + 1) * half] for i in range(4)], 0)
                for ref in (even, odd)
            ],
            1,
        )
        reads = read_ref[h]
        readouts.append(reads[:, CH:] + mm(reads[:, :CH], state))
    bonuses = [jnp.sum(weight[:, s], axis=1, keepdims=True) for s in slices]
    means = [jnp.mean(readout, axis=1, keepdims=True) for readout in readouts]
    centred = [readout - mean for readout, mean in zip(readouts, means)]
    spreads = [jnp.mean(c * c, axis=1, keepdims=True) for c in centred]
    scaled = [c * lax.rsqrt(spread + GROUP_EPS) for c, spread in zip(centred, spreads)]
    wide = (readouts[0].shape[0], CH)
    bonus = jnp.concatenate([jnp.broadcast_to(b, wide) for b in bonuses], 1)
    grouped = jnp.concatenate(scaled, 1) * gain_ref[...] + bias_ref[...]
    out = (grouped + bonus * v_ref[...].astype(F32)) * f_ref[...].astype(F32)
    out_ref[...] = out.astype(BF16)


def fetch(sources, targets, sems):
    copies = [
        pltpu.make_async_copy(source, target, sems.at[i])
        for i, (source, target) in enumerate(zip(sources, targets))
    ]
    for copy in copies:
        copy.start()
    return copies


def project_kernel(
    place_ref, token_ref, h0_ref, h1_ref, h2_ref, h3_ref, gain_ref, own_hbm, near_hbm, far_hbm,
    residual_hbm, out_ref, normed_ref, own_middle_ref, own_ref, near_ref, far_ref, residual_ref,
    wide_ref, rows_ref, sems,
):
    core = place_ref[1]
    tp = place_ref[2]
    copies = fetch(
        (own_hbm, near_hbm, far_hbm, residual_hbm), (own_ref, near_ref, far_ref, residual_ref), sems
    )
    copies[0].wait()
    acc = dot(h0_ref[...], own_ref[...])
    half = near_ref.shape[1]
    heads = [ref[...] for ref in (h1_ref, h2_ref, h3_ref)]
    copies[1].wait()
    for k, head in enumerate(heads):
        acc = acc + dot(jnp.where(core == 0, head[:, :half], head[:, half:]), near_ref[k])
    copies[2].wait()
    for k, head in enumerate(heads):
        acc = acc + dot(jnp.where(core == 0, head[:, half:], head[:, :half]), far_ref[k])
    copies[3].wait()
    middle = (residual_ref[...].astype(F32) + acc).astype(BF16)
    full = middle.astype(F32)
    scale = lax.rsqrt(jnp.mean(full * full, axis=1, keepdims=True) + NORM_EPS)
    normed = (full * scale * gain_ref[...]).astype(BF16)
    normed_ref[...] = normed
    cols = own_middle_ref.shape[1]
    own = middle[:, :cols]
    for y in range(1, middle.shape[1] // cols):
        own = jnp.where(tp == y, middle[:, y * cols : (y + 1) * cols], own)
    own_middle_ref[...] = own
    tiles = normed.shape[1] // LANES
    wide = normed.astype(F32)
    for i in range(tiles):
        wide_ref[:, i, :] = wide[:, i * LANES : (i + 1) * LANES]
    rows_ref[...] = wide_ref[:, :tiles, :].astype(BF16)
    dests = out_ref.shape[0] // (CAP * tiles)

    def send(i, carry):
        for m in range(CAP):
            token = jnp.maximum(token_ref[m, i * 4 + tp], 0)
            place = pl.multiple_of((i * CAP + m) * tiles, tiles)
            out_ref[pl.ds(place, tiles), :] = rows_ref[token]
        return carry

    lax.fori_loop(0, dests, send, 0, unroll=4)


def shared_kernel(place_ref, normed_ref, gate_ref, up_ref, down_ref, s0_ref, s1_ref, s2_ref, s3_ref):
    tp = place_ref[2]
    gate = dot(normed_ref[...], gate_ref[...])
    up = dot(normed_ref[...], up_ref[...])
    hidden = (gate * sigmoid(gate) * up).astype(BF16)
    cols = s0_ref.shape[1]
    for k, ref in enumerate((s0_ref, s1_ref, s2_ref, s3_ref)):
        start = pl.multiple_of(lax.rem(tp + k, 4) * cols, cols)
        ref[...] = dot(hidden, down_ref[:, pl.ds(start, cols)]).astype(ref.dtype)


def expert_kernel(
    rows_ref, gate_hbm, up_hbm, down_hbm, out_ref, gate_ref, up_ref, down_ref, wide_ref, x_ref, sems
):
    copies = fetch((gate_hbm, up_hbm, down_hbm), (gate_ref, up_ref, down_ref), sems)
    width = gate_ref.shape[0]
    tiles = width // LANES
    block = CAP * tiles
    sources = rows_ref.shape[0] // block

    def widen(i, carry):
        wide_ref[pl.ds(pl.multiple_of(i * PAD, 8), block), :] = rows_ref[
            pl.ds(pl.multiple_of(i * block, block), block), :
        ].astype(F32)
        return carry

    lax.fori_loop(0, sources, widen, 0, unroll=4)
    for m in range(CAP):
        for i in range(tiles):
            x_ref[m * sources : (m + 1) * sources, i * LANES : (i + 1) * LANES] = wide_ref[
                pl.ds(m * tiles + i, sources, stride=PAD), :
            ].astype(BF16)
    x = x_ref[...]
    copies[0].wait()
    gate = dot(x, gate_ref[...])
    copies[1].wait()
    up = dot(x, up_ref[...])
    hidden = (gate * sigmoid(gate) * up).astype(BF16)
    cols = width // 4
    copies[2].wait()
    for y in range(4):
        answer = dot(hidden, down_ref[:, y * cols : (y + 1) * cols])
        for m in range(CAP):
            for i in range(cols // LANES):
                place = (y * CAP + m) * (cols // LANES) + i
                wide_ref[pl.ds(place, sources, stride=PAD), :] = answer[
                    m * sources : (m + 1) * sources, i * LANES : (i + 1) * LANES
                ]

    def narrow(i, carry):
        out_ref[pl.ds(pl.multiple_of(i * block, block), block), :] = wide_ref[
            pl.ds(pl.multiple_of(i * PAD, 8), block), :
        ].astype(BF16)
        return carry

    lax.fori_loop(0, sources, narrow, 0, unroll=4)


def combine_kernel(
    back_ref, token_ref, weight_ref, middle_ref, s0_ref, s1_ref, s2_ref, s3_ref, out_ref, wide_ref
):
    tokens, cols = out_ref.shape
    tiles = cols // LANES
    slots, experts = token_ref.shape
    wide_ref[...] = back_ref[...].astype(F32)
    token, _ = iotas(tokens, experts)
    total = middle_ref[...].astype(F32) + s0_ref[...] + s1_ref[...].astype(F32)
    total = total + s2_ref[...].astype(F32) + s3_ref[...].astype(F32)
    tables, rows = [], []
    for m in range(slots):
        same = token_ref[m : m + 1, :] == token
        tables.append(jnp.where(same, weight_ref[m : m + 1, :], 0.0).astype(BF16))
        rows.append(
            jnp.concatenate(
                [
                    wide_ref[pl.ds(m * tiles + i, experts, stride=slots * tiles), :].astype(BF16)
                    for i in range(tiles)
                ],
                1,
            )
        )
    routed = dot(jnp.concatenate(tables, 1), jnp.concatenate(rows, 0))
    out_ref[...] = (total + routed).astype(BF16)


def call(kernel, out, *args, scalars=0, fetched=0, scratch=()):
    smem = pl.BlockSpec(memory_space=pltpu.SMEM)
    vmem = pl.BlockSpec(memory_space=pltpu.VMEM)
    hbm = pl.BlockSpec(memory_space=pl.ANY)
    loaded = len(args) - scalars - fetched
    scratch = list(scratch)
    if fetched:
        scratch = [pltpu.VMEM(a.shape, a.dtype) for a in args[-fetched:]] + scratch
        scratch.append(pltpu.SemaphoreType.DMA((fetched,)))
    return pl.pallas_call(
        kernel,
        out_shape=out,
        in_specs=[smem] * scalars + [vmem] * loaded + [hbm] * fetched,
        out_specs=jax.tree.map(lambda _: vmem, out),
        scratch_shapes=scratch,
    )(*args)


def exchange(array, axes):
    return lax.all_to_all(array, axes, split_axis=0, concat_axis=0, tiled=True)


def turned(array, axis, shift):
    peers = lax.axis_size(axis)
    return lax.ppermute(array, axis, [(i, (i + shift) % peers) for i in range(peers)])


def layer(
    receptance, key, value, decay, correction, factor, mix, current, gain, bias, output_matrix,
    residual, norm_gain, routes, chosen, routed_gate, routed_up, routed_down, common_gate,
    common_up, common_down,
):
    shape = jax.ShapeDtypeStruct
    tokens, inner = key.shape
    width = residual.shape[1]
    cols = width // 4
    heads = inner // CH
    z_count, plane = lax.axis_size("z"), lax.axis_size(PLANE)
    experts = lax.axis_size(EVERY)
    slots = lax.axis_size(SP) * CAP
    core = lax.axis_index("c")
    place = jnp.stack([lax.axis_index("z"), core, lax.axis_index("tp")]).astype(jnp.int32)
    mix, current, gain, bias = (a.reshape(1, -1) for a in (mix, current, gain, bias))

    maps, reads = call(
        local_kernel,
        (shape((2 * heads, 3 * CH // 4, 2 * CH), F32), shape((heads, tokens, 2 * CH), F32)),
        receptance, key, value, decay, correction, mix,
    )
    maps, output_rows = lax.optimization_barrier((maps, output_matrix))
    half = inner // 2
    maps = exchange(maps, PLANE)
    mine = lax.dynamic_slice_in_dim(output_rows, core * half, half, 0)
    near = [turned(mine, "tp", k) for k in (1, 2, 3)]
    before, totals = call(
        plane_kernel,
        (
            shape((plane, CH, 3 * CH // 2), F32),
            shape((z_count, 3 * CH // 4, 2 * CH), F32),
        ),
        maps,
    )
    totals = exchange(totals, "z")
    slot_token, slot_weight = call(
        routing_kernel,
        (shape((CAP, experts), jnp.int32), shape((CAP, experts), F32)), routes, chosen,
    )
    states = call(
        entering_kernel, shape((plane, CH // 4, 2 * CH), F32), place, before, totals,
        scalars=1,
    )
    states, *near = lax.optimization_barrier((states, *near))
    near = jnp.stack(near)
    far = turned(near, "c", 1)
    states = exchange(states, PLANE)
    mixed = call(
        finish_kernel, shape((tokens, inner), BF16), states, reads, receptance, key,
        value, correction, factor, mix, current, gain, bias,
    )
    others = [turned(mixed, "tp", k) for k in (1, 2, 3)]
    outgoing, normed, own_middle = call(
        project_kernel,
        (
            shape((slots * width // LANES, LANES), BF16),
            shape((tokens, width), BF16),
            shape((tokens, cols), BF16),
        ),
        place, slot_token, mixed, *others, norm_gain.reshape(1, -1), output_matrix, near, far,
        residual,
        scalars=2,
        fetched=4,
        scratch=(
            pltpu.VMEM((tokens, width // LANES + 8, LANES), F32),
            pltpu.VMEM((tokens, width // LANES, LANES), BF16),
        ),
    )
    arrived = exchange(outgoing, SP)
    shared = call(
        shared_kernel,
        (shape((tokens, cols), F32),) + (shape((tokens, cols), BF16),) * 3,
        place, normed, common_gate, common_up, common_down, scalars=1,
    )
    shared = [shared[0]] + [turned(shared[k], "tp", k) for k in (1, 2, 3)]
    answer = call(
        expert_kernel, shape(outgoing.shape, BF16), arrived, routed_gate[0],
        routed_up[0], routed_down[0],
        fetched=3,
        scratch=(
            pltpu.VMEM((slots // CAP * PAD, LANES), F32),
            pltpu.VMEM((slots, width), BF16),
        ),
    )
    back = exchange(answer, EVERY)
    return call(
        combine_kernel, shape((tokens, cols), BF16), back, slot_token, slot_weight,
        own_middle, *shared,
        scratch=(pltpu.VMEM(back.shape, F32),),
    )


def solution(mesh):
    finer = Mesh(mesh.devices.reshape(8, 4, 2, mesh.shape["tp"]), EVERY)
    placed = (
        (P(SP, "tp"),) * 6
        + (P("tp"),) * 4
        + (P("tp", None), P(SP, None), P(), P(SP, None), P(SP, None))
        + (P(EVERY, None, None),) * 3
        + (P(None, "tp"), P(None, "tp"), P("tp", None))
    )
    return jax.shard_map(layer, mesh=finer, in_specs=placed, out_specs=P(SP, "tp"), check_vma=False)
```

```python
import jax
import jax.numpy as jnp
from jax import lax
from jax.experimental import pallas as pl
from jax.experimental.pallas import tpu as pltpu
from jax.sharding import Mesh
from jax.sharding import PartitionSpec as P


CH = 64
CAP = 6
LANES = 128
NORM_EPS = 1e-06
GROUP_EPS = 0.00064
PLANE = ("x", "c")
SP = ("z", "x", "c")
EVERY = ("z", "x", "c", "tp")
F32 = jnp.float32
BF16 = jnp.bfloat16
NN = ((1,), (0,))
NT = ((1,), (1,))
TN = ((0,), (0,))
PAD = 104


def dot(a, b, dims=NN):
    return lax.dot_general(a, b, (dims, ((), ())), preferred_element_type=F32)


def split(a):
    high = a.astype(BF16)
    return high, (a - high.astype(F32)).astype(BF16)


def mm(a, b, dims=NN):
    ah, al = split(a)
    bh, bl = split(b)
    return dot(ah, bh, dims) + (dot(al, bh, dims) + dot(ah, bl, dims))


def iotas(rows, cols):
    return (
        lax.broadcasted_iota(jnp.int32, (rows, cols), 0),
        lax.broadcasted_iota(jnp.int32, (rows, cols), 1),
    )


def sigmoid(x):
    return 1.0 / (1.0 + jnp.exp(-x))


def unit_inverses(lows):
    n = lows[0].shape[0]
    row, col = iotas(n, n)
    size = 8
    eye = jnp.where(row == col, 1.0, 0.0)
    inside = (row // size) == (col // size)
    powers = [jnp.where(inside, low, 0.0) for low in lows]
    xs = [eye + power for power in powers]
    span = 2
    while span < size:
        powers = [mm(power, power) for power in powers]
        xs = [x + mm(x, power) for x, power in zip(xs, powers)]
        span *= 2
    while size < n:
        part = ((row // (2 * size)) == (col // (2 * size))) & ((row // size) != (col // size))
        lefts = [mm(x, jnp.where(part, low, 0.0)) for x, low in zip(xs, lows)]
        xs = [x + mm(left, x) for x, left in zip(xs, lefts)]
        size *= 2
    return xs


def mixed_of(key, learning, mix):
    return key * (1.0 + (learning - 1.0) * mix)


def routing_kernel(routes_ref, weight_ref, token_ref, slot_weight_ref):
    slots, experts = token_ref.shape
    tokens, top = routes_ref.shape
    token, expert = iotas(tokens, experts)
    weight = jnp.zeros((tokens, experts), F32)
    hit = jnp.zeros((tokens, experts), F32)
    for k in range(top):
        same = routes_ref[:, k : k + 1] == expert
        hit = jnp.where(same, 1.0, hit)
        weight = jnp.where(same, weight_ref[:, k : k + 1], weight)
    row, col = iotas(tokens, tokens)
    earlier = jnp.where(row > col, 1.0, 0.0).astype(BF16)
    within = dot(earlier, hit.astype(BF16))
    within = jnp.where(hit > 0.5, within, -1.0)
    number = token.astype(F32) + 1.0
    for m in range(slots):
        chosen = within == float(m)
        name = jnp.sum(jnp.where(chosen, number, 0.0), axis=0, keepdims=True) - 1.0
        token_ref[m : m + 1, :] = name.astype(jnp.int32)
        slot_weight_ref[m : m + 1, :] = jnp.sum(
            jnp.where(chosen, weight, 0.0), axis=0, keepdims=True
        )


def local_kernel(r_ref, k_ref, v_ref, d_ref, c_ref, mix_ref, map_ref, read_ref):
    t, w = k_ref.shape
    key = k_ref[...].astype(F32)
    learning = sigmoid(c_ref[...].astype(F32))
    log_decay = -0.6065306597126334 * sigmoid(d_ref[...].astype(F32))
    row, col = iotas(w, w)
    group = jnp.where(row // CH == col // CH, 1.0, 0.0).astype(BF16)
    square_high, square_low = split(key * key)
    length = jnp.sqrt(dot(square_high, group) + dot(square_low, group))
    unit = key / jnp.maximum(length, 1.0)
    mixed = mixed_of(key, learning, mix_ref[...])
    row, col = iotas(t, t)
    upto = jnp.where(row >= col, 1.0, 0.0).astype(BF16)
    first = log_decay.astype(BF16)
    second, third = split(log_decay - first.astype(F32))
    total = dot(upto, first) + (dot(upto, second) + dot(upto, third))
    last = total[t - 1 : t, :]
    value = v_ref[...].astype(F32)
    before = -jnp.exp(total - log_decay) * unit
    inverse_decay = jnp.exp(-total)
    rate = unit * learning
    erase = inverse_decay * rate
    write = inverse_decay * mixed
    read = jnp.exp(total) * r_ref[...].astype(F32)
    remaining = jnp.exp(last - total)
    erase_end = remaining * rate
    write_end = remaining * mixed
    final = jnp.exp(last)
    strict = row > col
    inclusive = row >= col
    hrow, hcol = iotas(CH, CH)
    every = range(w // CH)

    def parts(array):
        return [array[:, h * CH : (h + 1) * CH] for h in every]

    befores, asked, values = parts(before), parts(read), parts(value)
    pairs = [
        mm(jnp.concatenate([b, q], 0), jnp.concatenate([e, x], 0), NT)
        for b, q, e, x in zip(befores, asked, parts(erase), parts(write))
    ]
    lows = [jnp.where(strict, p[:t, :t], 0.0) for p in pairs]
    stacks = [
        jnp.concatenate(
            [jnp.where(strict, p[:t, t:], 0.0), jnp.where(inclusive, p[t:, t:], 0.0)], 0
        )
        for p in pairs
    ]
    on_values = [mm(stack, v) for stack, v in zip(stacks, values)]
    written = [mm(e, v, TN) for e, v in zip(parts(write_end), values)]
    xs = unit_inverses(lows)
    solved = [
        mm(x, jnp.concatenate([b, o[:t]], 1)) for x, b, o in zip(xs, befores, on_values)
    ]
    states = [mm(e, z, TN) for e, z in zip(parts(erase_end), solved)]
    reads = [mm(jnp.where(inclusive, p[t:, :t], 0.0), z) for p, z in zip(pairs, solved)]
    for h, f in zip(every, parts(final)):
        diagonal = jnp.where(hrow == hcol, jnp.broadcast_to(f, (CH, CH)), 0.0)
        state = states[h] + jnp.concatenate([diagonal, written[h]], 1)
        map_ref[2 * h], map_ref[2 * h + 1] = packed(state)
        read_ref[h] = reads[h] + jnp.concatenate([asked[h], on_values[h][t:]], 1)


def packed(state):
    half = CH // 2
    left = jnp.concatenate([state[:half, :CH], state[half:, :CH]], 1)
    quarter = half // 2
    pieces = []
    for c in range(2):
        cols = state[:, CH + c * half : CH + (c + 1) * half]
        rows = [cols[i * quarter : (i + 1) * quarter] for i in range(4)]
        pieces.append(jnp.concatenate([left, jnp.concatenate(rows, 1)], 0))
    return pieces


def repacked(state):
    half = CH // 2
    quarter = half // 2
    left = jnp.concatenate([state[:half, :CH], state[half:, :CH]], 1)
    rows = [state[i * quarter : (i + 1) * quarter, CH:] for i in range(4)]
    return jnp.concatenate([left, jnp.concatenate(rows, 1)], 0)


def unpacked(block):
    half = CH // 2
    left = jnp.concatenate([block[:half, :CH], block[:half, CH:]], 0)
    right = jnp.concatenate([block[half:, i * half : (i + 1) * half] for i in range(4)], 0)
    return jnp.concatenate([left, right], 1)


def joined(former, latter, late):
    return mm(latter[:, :CH], former) + jnp.where(late, latter, 0.0)


def plane_kernel(map_ref, before_ref, total_ref):
    count = map_ref.shape[0]
    hrow, hcol = iotas(CH, 3 * CH // 2)
    late = hcol >= CH
    maps = [unpacked(map_ref[q]) for q in range(count)]
    span = 1
    while span < count:
        maps = [
            maps[q] if q < span else joined(maps[q - span], maps[q], late) for q in range(count)
        ]
        span *= 2
    total = repacked(maps[count - 1])
    for z in range(total_ref.shape[0]):
        total_ref[z] = total
    before_ref[0] = jnp.where(hrow == hcol, 1.0, 0.0)
    for q in range(1, count):
        before_ref[q] = maps[q - 1]


def entering_kernel(place_ref, before_ref, total_ref, out_ref):
    z_here = place_ref[0]
    hrow, hcol = iotas(CH, 3 * CH // 2)
    late = hcol >= CH
    nothing = jnp.where(hrow == hcol, 1.0, 0.0)
    maps = [
        jnp.where(z < z_here, unpacked(total_ref[z]), nothing)
        for z in range(total_ref.shape[0] - 1)
    ]
    while len(maps) > 1:
        odd = maps[:1] if len(maps) % 2 else []
        rest = maps[len(odd) :]
        maps = odd + [
            joined(rest[i], rest[i + 1], late) for i in range(0, len(rest), 2)
        ]
    state = maps[0][:, CH:]
    count = before_ref.shape[0]
    rows = jnp.concatenate([before_ref[q] for q in range(count)], 0)
    mine = mm(rows[:, :CH], state) + rows[:, CH:]
    quarter = CH // 4
    for q in range(count):
        pieces = [mine[q * CH + i * quarter : q * CH + (i + 1) * quarter] for i in range(4)]
        out_ref[q] = jnp.concatenate(pieces, 1)


def finish_kernel(
    state_ref, read_ref, r_ref, k_ref, v_ref, c_ref, f_ref, mix_ref, cur_ref, gain_ref, bias_ref,
    out_ref,
):
    every = range(read_ref.shape[0])
    slices = [slice(h * CH, (h + 1) * CH) for h in every]
    mixed = mixed_of(k_ref[...].astype(F32), sigmoid(c_ref[...].astype(F32)), mix_ref[...])
    weight = r_ref[...].astype(F32) * mixed * cur_ref[...]
    readouts = []
    for h in every:
        even, odd = state_ref[2 * h], state_ref[2 * h + 1]
        half = CH // 2
        state = jnp.concatenate(
            [
                jnp.concatenate([ref[:, i * half : (i + 1) * half] for i in range(4)], 0)
                for ref in (even, odd)
            ],
            1,
        )
        reads = read_ref[h]
        readouts.append(reads[:, CH:] + mm(reads[:, :CH], state))
    bonuses = [jnp.sum(weight[:, s], axis=1, keepdims=True) for s in slices]
    means = [jnp.mean(readout, axis=1, keepdims=True) for readout in readouts]
    centred = [readout - mean for readout, mean in zip(readouts, means)]
    spreads = [jnp.mean(c * c, axis=1, keepdims=True) for c in centred]
    scaled = [c * lax.rsqrt(spread + GROUP_EPS) for c, spread in zip(centred, spreads)]
    wide = (readouts[0].shape[0], CH)
    bonus = jnp.concatenate([jnp.broadcast_to(b, wide) for b in bonuses], 1)
    grouped = jnp.concatenate(scaled, 1) * gain_ref[...] + bias_ref[...]
    out = (grouped + bonus * v_ref[...].astype(F32)) * f_ref[...].astype(F32)
    out = out.astype(BF16)
    for y in range(out_ref.shape[0]):
        out_ref[y] = out


def project_kernel(
    place_ref, token_ref, heads_ref, gain_ref, own_ref, near_ref, far_ref, residual_ref, out_ref,
    normed_ref, own_middle_ref, wide_ref, rows_ref,
):
    core = place_ref[1]
    tp = place_ref[2]
    acc = dot(heads_ref[tp], own_ref[...])
    half = near_ref.shape[1]
    for k in range(3):
        head = heads_ref[lax.rem(tp + 3 - k, 4)]
        low, high = head[:, :half], head[:, half:]
        acc = acc + dot(jnp.where(core == 0, low, high), near_ref[k])
        acc = acc + dot(jnp.where(core == 0, high, low), far_ref[k])
    middle = (residual_ref[...].astype(F32) + acc).astype(BF16)
    full = middle.astype(F32)
    scale = lax.rsqrt(jnp.mean(full * full, axis=1, keepdims=True) + NORM_EPS)
    normed = (full * scale * gain_ref[...]).astype(BF16)
    normed_ref[...] = normed
    cols = own_middle_ref.shape[1]
    own = middle[:, :cols]
    for y in range(1, middle.shape[1] // cols):
        own = jnp.where(tp == y, middle[:, y * cols : (y + 1) * cols], own)
    own_middle_ref[...] = own
    tiles = normed.shape[1] // LANES
    wide = normed.astype(F32)
    for i in range(tiles):
        wide_ref[:, i, :] = wide[:, i * LANES : (i + 1) * LANES]
    rows_ref[...] = wide_ref[:, :tiles, :].astype(BF16)
    dests = out_ref.shape[0] // (CAP * tiles)

    def send(i, carry):
        for m in range(CAP):
            token = jnp.maximum(token_ref[m, i * 4 + tp], 0)
            place = pl.multiple_of((i * CAP + m) * tiles, tiles)
            out_ref[pl.ds(place, tiles), :] = rows_ref[token]
        return carry

    lax.fori_loop(0, dests, send, 0, unroll=4)


def shared_kernel(place_ref, normed_ref, gate_ref, up_ref, down_ref, s0_ref, s1_ref, s2_ref, s3_ref):
    tp = place_ref[2]
    gate = dot(normed_ref[...], gate_ref[...])
    up = dot(normed_ref[...], up_ref[...])
    hidden = (gate * sigmoid(gate) * up).astype(BF16)
    cols = s0_ref.shape[1]
    for k, ref in enumerate((s0_ref, s1_ref, s2_ref, s3_ref)):
        start = pl.multiple_of(lax.rem(tp + k, 4) * cols, cols)
        ref[...] = dot(hidden, down_ref[:, pl.ds(start, cols)]).astype(ref.dtype)


def expert_kernel(rows_ref, gate_ref, up_ref, down_ref, out_ref, wide_ref, x_ref):
    width = gate_ref.shape[0]
    tiles = width // LANES
    block = CAP * tiles
    sources = rows_ref.shape[0] // block

    def widen(i, carry):
        wide_ref[pl.ds(pl.multiple_of(i * PAD, 8), block), :] = rows_ref[
            pl.ds(pl.multiple_of(i * block, block), block), :
        ].astype(F32)
        return carry

    lax.fori_loop(0, sources, widen, 0, unroll=4)
    for m in range(CAP):
        for i in range(tiles):
            x_ref[m * sources : (m + 1) * sources, i * LANES : (i + 1) * LANES] = wide_ref[
                pl.ds(m * tiles + i, sources, stride=PAD), :
            ].astype(BF16)
    x = x_ref[...]
    gate = dot(x, gate_ref[...])
    up = dot(x, up_ref[...])
    hidden = (gate * sigmoid(gate) * up).astype(BF16)
    cols = width // 4
    for y in range(4):
        answer = dot(hidden, down_ref[:, y * cols : (y + 1) * cols])
        for m in range(CAP):
            for i in range(cols // LANES):
                place = (y * CAP + m) * (cols // LANES) + i
                wide_ref[pl.ds(place, sources, stride=PAD), :] = answer[
                    m * sources : (m + 1) * sources, i * LANES : (i + 1) * LANES
                ]

    def narrow(i, carry):
        out_ref[pl.ds(pl.multiple_of(i * block, block), block), :] = wide_ref[
            pl.ds(pl.multiple_of(i * PAD, 8), block), :
        ].astype(BF16)
        return carry

    lax.fori_loop(0, sources, narrow, 0, unroll=4)


def combine_kernel(
    back_ref, token_ref, weight_ref, middle_ref, s0_ref, s1_ref, s2_ref, s3_ref, out_ref, wide_ref
):
    tokens, cols = out_ref.shape
    tiles = cols // LANES
    slots, experts = token_ref.shape
    wide_ref[...] = back_ref[...].astype(F32)
    token, _ = iotas(tokens, experts)
    total = middle_ref[...].astype(F32) + s0_ref[...] + s1_ref[...].astype(F32)
    total = total + s2_ref[...].astype(F32) + s3_ref[...].astype(F32)
    tables, rows = [], []
    for m in range(slots):
        same = token_ref[m : m + 1, :] == token
        tables.append(jnp.where(same, weight_ref[m : m + 1, :], 0.0).astype(BF16))
        rows.append(
            jnp.concatenate(
                [
                    wide_ref[pl.ds(m * tiles + i, experts, stride=slots * tiles), :].astype(BF16)
                    for i in range(tiles)
                ],
                1,
            )
        )
    routed = dot(jnp.concatenate(tables, 1), jnp.concatenate(rows, 0))
    out_ref[...] = (total + routed).astype(BF16)


def call(kernel, out, *args, scalars=0, scratch=(), limit=16, inside=True, kept=True):
    smem = pl.BlockSpec(memory_space=pltpu.SMEM)
    vmem = pl.BlockSpec(memory_space=pltpu.VMEM)
    args = list(args)
    space = pltpu.VMEM if inside else pltpu.HBM
    args[scalars:] = [pltpu.with_memory_space_constraint(a, space) for a in args[scalars:]]
    return pl.pallas_call(
        kernel,
        out_shape=jax.tree.map(lambda a: pltpu.VMEM(a.shape, a.dtype), out) if kept else out,
        in_specs=[smem] * scalars + [vmem] * (len(args) - scalars),
        out_specs=jax.tree.map(lambda _: vmem, out),
        scratch_shapes=list(scratch),
        compiler_params=pltpu.CompilerParams(vmem_limit_bytes=limit << 20),
    )(*args)


def exchange(array, axes):
    return lax.all_to_all(array, axes, split_axis=0, concat_axis=0, tiled=True)


def turned(array, axis, shift):
    peers = lax.axis_size(axis)
    return lax.ppermute(array, axis, [(i, (i + shift) % peers) for i in range(peers)])


def layer(
    receptance, key, value, decay, correction, factor, mix, current, gain, bias, output_matrix,
    residual, norm_gain, routes, chosen, routed_gate, routed_up, routed_down, common_gate,
    common_up, common_down,
):
    shape = jax.ShapeDtypeStruct
    tokens, inner = key.shape
    width = residual.shape[1]
    cols = width // 4
    heads = inner // CH
    z_count, plane = lax.axis_size("z"), lax.axis_size(PLANE)
    experts = lax.axis_size(EVERY)
    slots = lax.axis_size(SP) * CAP
    core = lax.axis_index("c")
    place = jnp.stack([lax.axis_index("z"), core, lax.axis_index("tp")]).astype(jnp.int32)
    mix, current, gain, bias = (a.reshape(1, -1) for a in (mix, current, gain, bias))

    maps, reads = call(
        local_kernel,
        (shape((2 * heads, 3 * CH // 4, 2 * CH), F32), shape((heads, tokens, 2 * CH), F32)),
        receptance, key, value, decay, correction, mix, inside=False,
    )
    maps, output_rows = lax.optimization_barrier((maps, output_matrix))
    half = inner // 2
    maps = exchange(maps, PLANE)
    mine = lax.dynamic_slice_in_dim(output_rows, core * half, half, 0)
    near = [turned(mine, "tp", k) for k in (1, 2, 3)]
    before, totals = call(
        plane_kernel,
        (
            shape((plane, CH, 3 * CH // 2), F32),
            shape((z_count, 3 * CH // 4, 2 * CH), F32),
        ),
        maps,
    )
    totals = exchange(totals, "z")
    slot_token, slot_weight = call(
        routing_kernel,
        (shape((CAP, experts), jnp.int32), shape((CAP, experts), F32)), routes, chosen,
    )
    states = call(
        entering_kernel, shape((plane, CH // 4, 2 * CH), F32), place, before, totals,
        scalars=1,
    )
    states, *near = lax.optimization_barrier((states, *near))
    near = jnp.stack(near)
    far = turned(near, "c", 1)
    states = exchange(states, PLANE)
    mixed = call(
        finish_kernel, shape((4, tokens, inner), BF16), states, reads, receptance, key,
        value, correction, factor, mix, current, gain, bias,
    )
    mixed = exchange(mixed, "tp")
    outgoing, normed, own_middle = call(
        project_kernel,
        (
            shape((slots * width // LANES, LANES), BF16),
            shape((tokens, width), BF16),
            shape((tokens, cols), BF16),
        ),
        place, slot_token, mixed, norm_gain.reshape(1, -1), output_matrix, near, far, residual,
        scalars=2,
        scratch=(
            pltpu.VMEM((tokens, width // LANES + 8, LANES), F32),
            pltpu.VMEM((tokens, width // LANES, LANES), BF16),
        ),
    )
    arrived = exchange(outgoing, SP)
    shared = call(
        shared_kernel,
        (shape((tokens, cols), F32),) + (shape((tokens, cols), BF16),) * 3,
        place, normed, common_gate, common_up, common_down, scalars=1,
    )
    shared = [shared[0]] + [turned(shared[k], "tp", k) for k in (1, 2, 3)]
    answer = call(
        expert_kernel, shape(outgoing.shape, BF16), arrived, routed_gate[0],
        routed_up[0], routed_down[0],
        scratch=(
            pltpu.VMEM((slots // CAP * PAD, LANES), F32),
            pltpu.VMEM((slots, width), BF16),
        ),
    )
    back = exchange(answer, EVERY)
    return call(
        combine_kernel, shape((tokens, cols), BF16), back, slot_token, slot_weight,
        own_middle, *shared,
        scratch=(pltpu.VMEM(back.shape, F32),), kept=False,
    )


def solution(mesh):
    finer = Mesh(mesh.devices.reshape(8, 4, 2, mesh.shape["tp"]), EVERY)
    placed = (
        (P(SP, "tp"),) * 6
        + (P("tp"),) * 4
        + (P("tp", None), P(SP, None), P(), P(SP, None), P(SP, None))
        + (P(EVERY, None, None),) * 3
        + (P(None, "tp"), P(None, "tp"), P("tp", None))
    )
    return jax.shard_map(layer, mesh=finer, in_specs=placed, out_specs=P(SP, "tp"), check_vma=False)
```

```python
import jax
import jax.numpy as jnp
from jax import lax
from jax.experimental import pallas as pl
from jax.experimental.pallas import tpu as pltpu
from jax.sharding import Mesh
from jax.sharding import PartitionSpec as P


CH = 64
CAP = 6
LANES = 128
NORM_EPS = 1e-06
GROUP_EPS = 0.00064
PLANE = ("x", "c")
SP = ("z", "x", "c")
EVERY = ("z", "x", "c", "tp")
F32 = jnp.float32
BF16 = jnp.bfloat16
NN = ((1,), (0,))
NT = ((1,), (1,))
TN = ((0,), (0,))
PAD = 104


def dot(a, b, dims=NN):
    return lax.dot_general(a, b, (dims, ((), ())), preferred_element_type=F32)


def split(a):
    high = a.astype(BF16)
    return high, (a - high.astype(F32)).astype(BF16)


def mm(a, b, dims=NN):
    ah, al = split(a)
    bh, bl = split(b)
    return dot(ah, bh, dims) + (dot(al, bh, dims) + dot(ah, bl, dims))


def iotas(rows, cols):
    return (
        lax.broadcasted_iota(jnp.int32, (rows, cols), 0),
        lax.broadcasted_iota(jnp.int32, (rows, cols), 1),
    )


def sigmoid(x):
    return 1.0 / (1.0 + jnp.exp(-x))


def unit_inverses(lows):
    n = lows[0].shape[0]
    row, col = iotas(n, n)
    size = 8
    eye = jnp.where(row == col, 1.0, 0.0)
    inside = (row // size) == (col // size)
    powers = [jnp.where(inside, low, 0.0) for low in lows]
    xs = [eye + power for power in powers]
    span = 2
    while span < size:
        powers = [mm(power, power) for power in powers]
        xs = [x + mm(x, power) for x, power in zip(xs, powers)]
        span *= 2
    while size < n:
        part = ((row // (2 * size)) == (col // (2 * size))) & ((row // size) != (col // size))
        lefts = [mm(x, jnp.where(part, low, 0.0)) for x, low in zip(xs, lows)]
        xs = [x + mm(left, x) for x, left in zip(xs, lefts)]
        size *= 2
    return xs


def mixed_of(key, learning, mix):
    return key * (1.0 + (learning - 1.0) * mix)


def routing_kernel(routes_ref, weight_ref, token_ref, slot_weight_ref):
    slots, experts = token_ref.shape
    tokens, top = routes_ref.shape
    token, expert = iotas(tokens, experts)
    weight = jnp.zeros((tokens, experts), F32)
    hit = jnp.zeros((tokens, experts), F32)
    for k in range(top):
        same = routes_ref[:, k : k + 1] == expert
        hit = jnp.where(same, 1.0, hit)
        weight = jnp.where(same, weight_ref[:, k : k + 1], weight)
    row, col = iotas(tokens, tokens)
    earlier = jnp.where(row > col, 1.0, 0.0).astype(BF16)
    within = dot(earlier, hit.astype(BF16))
    within = jnp.where(hit > 0.5, within, -1.0)
    number = token.astype(F32) + 1.0
    for m in range(slots):
        chosen = within == float(m)
        name = jnp.sum(jnp.where(chosen, number, 0.0), axis=0, keepdims=True) - 1.0
        token_ref[m : m + 1, :] = name.astype(jnp.int32)
        slot_weight_ref[m : m + 1, :] = jnp.sum(
            jnp.where(chosen, weight, 0.0), axis=0, keepdims=True
        )


def local_kernel(r_ref, k_ref, v_ref, d_ref, c_ref, mix_ref, map_ref, read_ref):
    t, w = k_ref.shape
    key = k_ref[...].astype(F32)
    learning = sigmoid(c_ref[...].astype(F32))
    log_decay = -0.6065306597126334 * sigmoid(d_ref[...].astype(F32))
    row, col = iotas(w, w)
    group = jnp.where(row // CH == col // CH, 1.0, 0.0).astype(BF16)
    square_high, square_low = split(key * key)
    length = jnp.sqrt(dot(square_high, group) + dot(square_low, group))
    unit = key / jnp.maximum(length, 1.0)
    mixed = mixed_of(key, learning, mix_ref[...])
    row, col = iotas(t, t)
    upto = jnp.where(row >= col, 1.0, 0.0).astype(BF16)
    first = log_decay.astype(BF16)
    second, third = split(log_decay - first.astype(F32))
    total = dot(upto, first) + (dot(upto, second) + dot(upto, third))
    last = total[t - 1 : t, :]
    value = v_ref[...].astype(F32)
    before = -jnp.exp(total - log_decay) * unit
    inverse_decay = jnp.exp(-total)
    rate = unit * learning
    erase = inverse_decay * rate
    write = inverse_decay * mixed
    read = jnp.exp(total) * r_ref[...].astype(F32)
    remaining = jnp.exp(last - total)
    erase_end = remaining * rate
    write_end = remaining * mixed
    final = jnp.exp(last)
    strict = row > col
    inclusive = row >= col
    hrow, hcol = iotas(CH, CH)
    every = range(w // CH)

    def parts(array):
        return [array[:, h * CH : (h + 1) * CH] for h in every]

    befores, asked, values = parts(before), parts(read), parts(value)
    pairs = [
        mm(jnp.concatenate([b, q], 0), jnp.concatenate([e, x], 0), NT)
        for b, q, e, x in zip(befores, asked, parts(erase), parts(write))
    ]
    lows = [jnp.where(strict, p[:t, :t], 0.0) for p in pairs]
    stacks = [
        jnp.concatenate(
            [jnp.where(strict, p[:t, t:], 0.0), jnp.where(inclusive, p[t:, t:], 0.0)], 0
        )
        for p in pairs
    ]
    on_values = [mm(stack, v) for stack, v in zip(stacks, values)]
    written = [mm(e, v, TN) for e, v in zip(parts(write_end), values)]
    xs = unit_inverses(lows)
    solved = [
        mm(x, jnp.concatenate([b, o[:t]], 1)) for x, b, o in zip(xs, befores, on_values)
    ]
    states = [mm(e, z, TN) for e, z in zip(parts(erase_end), solved)]
    reads = [mm(jnp.where(inclusive, p[t:, :t], 0.0), z) for p, z in zip(pairs, solved)]
    for h, f in zip(every, parts(final)):
        diagonal = jnp.where(hrow == hcol, jnp.broadcast_to(f, (CH, CH)), 0.0)
        state = states[h] + jnp.concatenate([diagonal, written[h]], 1)
        map_ref[2 * h], map_ref[2 * h + 1] = packed(state)
        read_ref[h] = reads[h] + jnp.concatenate([asked[h], on_values[h][t:]], 1)


def eye_of(width):
    row, col = iotas(CH, width)
    return jnp.where(row == col, 1.0, 0.0)


def folded(state, cols):
    half = CH // 2
    quarter = half // 2
    moved = state[:, :CH] - eye_of(CH)
    left = jnp.concatenate([moved[:half], moved[half:]], 1)
    rows = [state[i * quarter : (i + 1) * quarter, cols] for i in range(4)]
    return jnp.concatenate([left, jnp.concatenate(rows, 1)], 0).astype(BF16)


def packed(state):
    return [folded(state, slice(CH + c * CH // 2, CH + (c + 1) * CH // 2)) for c in range(2)]


def repacked(state):
    return folded(state, slice(CH, None))


def unpacked(block):
    half = CH // 2
    block = block.astype(F32)
    left = jnp.concatenate([block[:half, :CH], block[:half, CH:]], 0) + eye_of(CH)
    right = jnp.concatenate([block[half:, i * half : (i + 1) * half] for i in range(4)], 0)
    return jnp.concatenate([left, right], 1)


def joined(former, latter, late):
    return mm(latter[:, :CH], former) + jnp.where(late, latter, 0.0)


def plane_kernel(map_ref, before_ref, total_ref):
    count = map_ref.shape[0]
    hrow, hcol = iotas(CH, 3 * CH // 2)
    late = hcol >= CH
    maps = [unpacked(map_ref[q]) for q in range(count)]
    span = 1
    while span < count:
        maps = [
            maps[q] if q < span else joined(maps[q - span], maps[q], late) for q in range(count)
        ]
        span *= 2
    total = repacked(maps[count - 1])
    for z in range(total_ref.shape[0]):
        total_ref[z] = total
    before_ref[0] = jnp.where(hrow == hcol, 1.0, 0.0)
    for q in range(1, count):
        before_ref[q] = maps[q - 1]


def entering_kernel(place_ref, before_ref, total_ref, out_ref):
    z_here = place_ref[0]
    hrow, hcol = iotas(CH, 3 * CH // 2)
    late = hcol >= CH
    nothing = jnp.where(hrow == hcol, 1.0, 0.0)
    maps = [
        jnp.where(z < z_here, unpacked(total_ref[z]), nothing)
        for z in range(total_ref.shape[0] - 1)
    ]
    while len(maps) > 1:
        odd = maps[:1] if len(maps) % 2 else []
        rest = maps[len(odd) :]
        maps = odd + [
            joined(rest[i], rest[i + 1], late) for i in range(0, len(rest), 2)
        ]
    state = maps[0][:, CH:]
    count = before_ref.shape[0]
    rows = jnp.concatenate([before_ref[q] for q in range(count)], 0)
    mine = mm(rows[:, :CH], state) + rows[:, CH:]
    quarter = CH // 4
    for q in range(count):
        pieces = [mine[q * CH + i * quarter : q * CH + (i + 1) * quarter] for i in range(4)]
        out_ref[q] = jnp.concatenate(pieces, 1)


def finish_kernel(
    state_ref, read_ref, r_ref, k_ref, v_ref, c_ref, f_ref, mix_ref, cur_ref, gain_ref, bias_ref,
    out_ref,
):
    every = range(read_ref.shape[0])
    slices = [slice(h * CH, (h + 1) * CH) for h in every]
    mixed = mixed_of(k_ref[...].astype(F32), sigmoid(c_ref[...].astype(F32)), mix_ref[...])
    weight = r_ref[...].astype(F32) * mixed * cur_ref[...]
    readouts = []
    for h in every:
        even, odd = state_ref[2 * h], state_ref[2 * h + 1]
        half = CH // 2
        state = jnp.concatenate(
            [
                jnp.concatenate([ref[:, i * half : (i + 1) * half] for i in range(4)], 0)
                for ref in (even, odd)
            ],
            1,
        )
        reads = read_ref[h]
        readouts.append(reads[:, CH:] + mm(reads[:, :CH], state))
    bonuses = [jnp.sum(weight[:, s], axis=1, keepdims=True) for s in slices]
    means = [jnp.mean(readout, axis=1, keepdims=True) for readout in readouts]
    centred = [readout - mean for readout, mean in zip(readouts, means)]
    spreads = [jnp.mean(c * c, axis=1, keepdims=True) for c in centred]
    scaled = [c * lax.rsqrt(spread + GROUP_EPS) for c, spread in zip(centred, spreads)]
    wide = (readouts[0].shape[0], CH)
    bonus = jnp.concatenate([jnp.broadcast_to(b, wide) for b in bonuses], 1)
    grouped = jnp.concatenate(scaled, 1) * gain_ref[...] + bias_ref[...]
    out = (grouped + bonus * v_ref[...].astype(F32)) * f_ref[...].astype(F32)
    out = out.astype(BF16)
    for y in range(out_ref.shape[0]):
        out_ref[y] = out


def project_kernel(
    place_ref, token_ref, heads_ref, gain_ref, own_ref, near_ref, far_ref, residual_ref, out_ref,
    normed_ref, own_middle_ref, wide_ref, rows_ref,
):
    core = place_ref[1]
    tp = place_ref[2]
    half = near_ref.shape[1]
    width = residual_ref.shape[1]
    heads = [heads_ref[tp]]
    for k in range(3):
        head = heads_ref[lax.rem(tp + 3 - k, 4)]
        low, high = head[:, :half], head[:, half:]
        heads += [jnp.where(core == 0, low, high), jnp.where(core == 0, high, low)]
    pieces = []
    squares = jnp.zeros((heads[0].shape[0], LANES), F32)
    step = 2 * LANES
    for start in range(0, width, step):
        s = slice(start, start + step)
        acc = residual_ref[:, s].astype(F32) + dot(heads[0], own_ref[:, s])
        for k in range(3):
            acc = acc + dot(heads[2 * k + 1], near_ref[k, :, s])
            acc = acc + dot(heads[2 * k + 2], far_ref[k, :, s])
        piece = acc.astype(BF16)
        full = piece.astype(F32)
        squares = squares + full[:, :LANES] * full[:, :LANES] + full[:, LANES:] * full[:, LANES:]
        pieces.append(piece)
    middle = jnp.concatenate(pieces, 1)
    full = middle.astype(F32)
    scale = lax.rsqrt(jnp.sum(squares, axis=1, keepdims=True) / width + NORM_EPS)
    normed = (full * scale * gain_ref[...]).astype(BF16)
    normed_ref[...] = normed
    cols = own_middle_ref.shape[1]
    own = middle[:, :cols]
    for y in range(1, middle.shape[1] // cols):
        own = jnp.where(tp == y, middle[:, y * cols : (y + 1) * cols], own)
    own_middle_ref[...] = own
    tiles = normed.shape[1] // LANES
    wide = normed.astype(F32)
    for i in range(tiles):
        wide_ref[:, i, :] = wide[:, i * LANES : (i + 1) * LANES]
    rows_ref[...] = wide_ref[:, :tiles, :].astype(BF16)
    dests = out_ref.shape[0] // (CAP * tiles)

    def send(i, carry):
        for m in range(CAP):
            token = jnp.maximum(token_ref[m, i * 4 + tp], 0)
            place = pl.multiple_of((i * CAP + m) * tiles, tiles)
            out_ref[pl.ds(place, tiles), :] = rows_ref[token]
        return carry

    lax.fori_loop(0, dests, send, 0, unroll=4)


def shared_kernel(place_ref, normed_ref, gate_ref, up_ref, down_ref, s0_ref, s1_ref, s2_ref, s3_ref):
    tp = place_ref[2]
    gate = dot(normed_ref[...], gate_ref[...])
    up = dot(normed_ref[...], up_ref[...])
    hidden = (gate * sigmoid(gate) * up).astype(BF16)
    cols = s0_ref.shape[1]
    for k, ref in enumerate((s0_ref, s1_ref, s2_ref, s3_ref)):
        start = pl.multiple_of(lax.rem(tp + k, 4) * cols, cols)
        ref[...] = dot(hidden, down_ref[:, pl.ds(start, cols)]).astype(ref.dtype)


def expert_kernel(rows_ref, gate_ref, up_ref, down_ref, out_ref, wide_ref, x_ref):
    width = gate_ref.shape[0]
    tiles = width // LANES
    block = CAP * tiles
    sources = rows_ref.shape[0] // block

    def widen(i, carry):
        wide_ref[pl.ds(pl.multiple_of(i * PAD, 8), block), :] = rows_ref[
            pl.ds(pl.multiple_of(i * block, block), block), :
        ].astype(F32)
        return carry

    lax.fori_loop(0, sources, widen, 0, unroll=4)
    for m in range(CAP):
        for i in range(tiles):
            x_ref[m * sources : (m + 1) * sources, i * LANES : (i + 1) * LANES] = wide_ref[
                pl.ds(m * tiles + i, sources, stride=PAD), :
            ].astype(BF16)
    x = x_ref[...]
    gate = dot(x, gate_ref[...])
    up = dot(x, up_ref[...])
    hidden = (gate * sigmoid(gate) * up).astype(BF16)
    cols = width // 4
    for y in range(4):
        answer = dot(hidden, down_ref[:, y * cols : (y + 1) * cols])
        for m in range(CAP):
            for i in range(cols // LANES):
                place = (y * CAP + m) * (cols // LANES) + i
                wide_ref[pl.ds(place, sources, stride=PAD), :] = answer[
                    m * sources : (m + 1) * sources, i * LANES : (i + 1) * LANES
                ]

    def narrow(i, carry):
        out_ref[pl.ds(pl.multiple_of(i * block, block), block), :] = wide_ref[
            pl.ds(pl.multiple_of(i * PAD, 8), block), :
        ].astype(BF16)
        return carry

    lax.fori_loop(0, sources, narrow, 0, unroll=4)


def combine_kernel(
    back_ref, token_ref, weight_ref, middle_ref, s0_ref, s1_ref, s2_ref, s3_ref, out_ref, wide_ref
):
    tokens, cols = out_ref.shape
    tiles = cols // LANES
    slots, experts = token_ref.shape
    wide_ref[...] = back_ref[...].astype(F32)
    token, _ = iotas(tokens, experts)
    total = middle_ref[...].astype(F32) + s0_ref[...] + s1_ref[...].astype(F32)
    total = total + s2_ref[...].astype(F32) + s3_ref[...].astype(F32)
    tables, rows = [], []
    for m in range(slots):
        same = token_ref[m : m + 1, :] == token
        tables.append(jnp.where(same, weight_ref[m : m + 1, :], 0.0).astype(BF16))
        rows.append(
            jnp.concatenate(
                [
                    wide_ref[pl.ds(m * tiles + i, experts, stride=slots * tiles), :].astype(BF16)
                    for i in range(tiles)
                ],
                1,
            )
        )
    routed = dot(jnp.concatenate(tables, 1), jnp.concatenate(rows, 0))
    out_ref[...] = (total + routed).astype(BF16)


def call(kernel, out, *args, scalars=0, scratch=(), limit=16, inside=True, kept=True):
    smem = pl.BlockSpec(memory_space=pltpu.SMEM)
    vmem = pl.BlockSpec(memory_space=pltpu.VMEM)
    args = list(args)
    space = pltpu.VMEM if inside else pltpu.HBM
    args[scalars:] = [pltpu.with_memory_space_constraint(a, space) for a in args[scalars:]]
    return pl.pallas_call(
        kernel,
        out_shape=jax.tree.map(lambda a: pltpu.VMEM(a.shape, a.dtype), out) if kept else out,
        in_specs=[smem] * scalars + [vmem] * (len(args) - scalars),
        out_specs=jax.tree.map(lambda _: vmem, out),
        scratch_shapes=list(scratch),
        compiler_params=pltpu.CompilerParams(vmem_limit_bytes=limit << 20),
    )(*args)


def exchange(array, axes):
    return lax.all_to_all(array, axes, split_axis=0, concat_axis=0, tiled=True)


def turned(array, axis, shift):
    peers = lax.axis_size(axis)
    return lax.ppermute(array, axis, [(i, (i + shift) % peers) for i in range(peers)])


def layer(
    receptance, key, value, decay, correction, factor, mix, current, gain, bias, output_matrix,
    residual, norm_gain, routes, chosen, routed_gate, routed_up, routed_down, common_gate,
    common_up, common_down,
):
    shape = jax.ShapeDtypeStruct
    tokens, inner = key.shape
    width = residual.shape[1]
    cols = width // 4
    heads = inner // CH
    z_count, plane = lax.axis_size("z"), lax.axis_size(PLANE)
    experts = lax.axis_size(EVERY)
    slots = lax.axis_size(SP) * CAP
    core = lax.axis_index("c")
    place = jnp.stack([lax.axis_index("z"), core, lax.axis_index("tp")]).astype(jnp.int32)
    mix, current, gain, bias = (a.reshape(1, -1) for a in (mix, current, gain, bias))

    maps, reads = call(
        local_kernel,
        (shape((2 * heads, 3 * CH // 4, 2 * CH), BF16), shape((heads, tokens, 2 * CH), F32)),
        receptance, key, value, decay, correction, mix, inside=False,
    )
    maps, output_rows = lax.optimization_barrier((maps, output_matrix))
    half = inner // 2
    maps = exchange(maps, PLANE)
    mine = lax.dynamic_slice_in_dim(output_rows, core * half, half, 0)
    near = [turned(mine, "tp", k) for k in (1, 2, 3)]
    before, totals = call(
        plane_kernel,
        (
            shape((plane, CH, 3 * CH // 2), F32),
            shape((z_count, 3 * CH // 4, 2 * CH), BF16),
        ),
        maps,
    )
    totals = exchange(totals, "z")
    slot_token, slot_weight = call(
        routing_kernel,
        (shape((CAP, experts), jnp.int32), shape((CAP, experts), F32)), routes, chosen,
    )
    states = call(
        entering_kernel, shape((plane, CH // 4, 2 * CH), F32), place, before, totals,
        scalars=1,
    )
    states = exchange(states, PLANE)
    states, *near = lax.optimization_barrier((states, *near))
    near = jnp.stack(near)
    far = turned(near, "c", 1)
    mixed = call(
        finish_kernel, shape((4, tokens, inner), BF16), states, reads, receptance, key,
        value, correction, factor, mix, current, gain, bias,
    )
    mixed = exchange(mixed, "tp")
    outgoing, normed, own_middle = call(
        project_kernel,
        (
            shape((slots * width // LANES, LANES), BF16),
            shape((tokens, width), BF16),
            shape((tokens, cols), BF16),
        ),
        place, slot_token, mixed, norm_gain.reshape(1, -1), output_matrix, near, far, residual,
        scalars=2,
        scratch=(
            pltpu.VMEM((tokens, width // LANES + 8, LANES), F32),
            pltpu.VMEM((tokens, width // LANES, LANES), BF16),
        ),
    )
    arrived = exchange(outgoing, SP)
    shared = call(
        shared_kernel,
        (shape((tokens, cols), F32),) + (shape((tokens, cols), BF16),) * 3,
        place, normed, common_gate, common_up, common_down, scalars=1,
    )
    shared = [shared[0]] + [turned(shared[k], "tp", k) for k in (1, 2, 3)]
    answer = call(
        expert_kernel, shape(outgoing.shape, BF16), arrived, routed_gate[0],
        routed_up[0], routed_down[0],
        scratch=(
            pltpu.VMEM((slots // CAP * PAD, LANES), F32),
            pltpu.VMEM((slots, width), BF16),
        ),
    )
    back = exchange(answer, EVERY)
    return call(
        combine_kernel, shape((tokens, cols), BF16), back, slot_token, slot_weight,
        own_middle, *shared,
        scratch=(pltpu.VMEM(back.shape, F32),), kept=False,
    )


def solution(mesh):
    finer = Mesh(mesh.devices.reshape(8, 4, 2, mesh.shape["tp"]), EVERY)
    placed = (
        (P(SP, "tp"),) * 6
        + (P("tp"),) * 4
        + (P("tp", None), P(SP, None), P(), P(SP, None), P(SP, None))
        + (P(EVERY, None, None),) * 3
        + (P(None, "tp"), P(None, "tp"), P("tp", None))
    )
    return jax.shard_map(layer, mesh=finer, in_specs=placed, out_specs=P(SP, "tp"), check_vma=False)
```

```python
import jax
import jax.numpy as jnp
from jax import lax
from jax.experimental import pallas as pl
from jax.experimental.pallas import tpu as pltpu
from jax.sharding import Mesh
from jax.sharding import PartitionSpec as P


CH = 64
CAP = 6
LANES = 128
NORM_EPS = 1e-06
GROUP_EPS = 0.00064
PLANE = ("x", "c")
SP = ("z", "x", "c")
EVERY = ("z", "x", "c", "tp")
F32 = jnp.float32
BF16 = jnp.bfloat16
NN = ((1,), (0,))
NT = ((1,), (1,))
TN = ((0,), (0,))
PAD = 104


def dot(a, b, dims=NN):
    return lax.dot_general(a, b, (dims, ((), ())), preferred_element_type=F32)


def split(a):
    high = a.astype(BF16)
    return high, (a - high.astype(F32)).astype(BF16)


def mm(a, b, dims=NN):
    ah, al = split(a)
    bh, bl = split(b)
    return dot(ah, bh, dims) + (dot(al, bh, dims) + dot(ah, bl, dims))


def iotas(rows, cols):
    return (
        lax.broadcasted_iota(jnp.int32, (rows, cols), 0),
        lax.broadcasted_iota(jnp.int32, (rows, cols), 1),
    )


def sigmoid(x):
    return 1.0 / (1.0 + jnp.exp(-x))


def unit_inverses(lows):
    n = lows[0].shape[0]
    row, col = iotas(n, n)
    size = 8
    eye = jnp.where(row == col, 1.0, 0.0)
    inside = (row // size) == (col // size)
    powers = [jnp.where(inside, low, 0.0) for low in lows]
    xs = [eye + power for power in powers]
    span = 2
    while span < size:
        powers = [mm(power, power) for power in powers]
        xs = [x + mm(x, power) for x, power in zip(xs, powers)]
        span *= 2
    while size < n:
        part = ((row // (2 * size)) == (col // (2 * size))) & ((row // size) != (col // size))
        lefts = [mm(x, jnp.where(part, low, 0.0)) for x, low in zip(xs, lows)]
        xs = [x + mm(left, x) for x, left in zip(xs, lefts)]
        size *= 2
    return xs


def mixed_of(key, learning, mix):
    return key * (1.0 + (learning - 1.0) * mix)


def routing_kernel(routes_ref, weight_ref, token_ref, slot_weight_ref):
    slots, experts = token_ref.shape
    tokens, top = routes_ref.shape
    token, expert = iotas(tokens, experts)
    weight = jnp.zeros((tokens, experts), F32)
    hit = jnp.zeros((tokens, experts), F32)
    for k in range(top):
        same = routes_ref[:, k : k + 1] == expert
        hit = jnp.where(same, 1.0, hit)
        weight = jnp.where(same, weight_ref[:, k : k + 1], weight)
    row, col = iotas(tokens, tokens)
    earlier = jnp.where(row > col, 1.0, 0.0).astype(BF16)
    within = dot(earlier, hit.astype(BF16))
    within = jnp.where(hit > 0.5, within, -1.0)
    number = token.astype(F32) + 1.0
    for m in range(slots):
        chosen = within == float(m)
        name = jnp.sum(jnp.where(chosen, number, 0.0), axis=0, keepdims=True) - 1.0
        token_ref[m : m + 1, :] = name.astype(jnp.int32)
        slot_weight_ref[m : m + 1, :] = jnp.sum(
            jnp.where(chosen, weight, 0.0), axis=0, keepdims=True
        )


def local_kernel(r_ref, k_ref, v_ref, d_ref, c_ref, mix_ref, map_ref, read_ref):
    t, w = k_ref.shape
    key = k_ref[...].astype(F32)
    learning = sigmoid(c_ref[...].astype(F32))
    log_decay = -0.6065306597126334 * sigmoid(d_ref[...].astype(F32))
    row, col = iotas(w, w)
    group = jnp.where(row // CH == col // CH, 1.0, 0.0).astype(BF16)
    square_high, square_low = split(key * key)
    length = jnp.sqrt(dot(square_high, group) + dot(square_low, group))
    unit = key / jnp.maximum(length, 1.0)
    mixed = mixed_of(key, learning, mix_ref[...])
    row, col = iotas(t, t)
    upto = jnp.where(row >= col, 1.0, 0.0).astype(BF16)
    first = log_decay.astype(BF16)
    second, third = split(log_decay - first.astype(F32))
    total = dot(upto, first) + (dot(upto, second) + dot(upto, third))
    last = total[t - 1 : t, :]
    value = v_ref[...].astype(F32)
    before = -jnp.exp(total - log_decay) * unit
    inverse_decay = jnp.exp(-total)
    rate = unit * learning
    erase = inverse_decay * rate
    write = inverse_decay * mixed
    read = jnp.exp(total) * r_ref[...].astype(F32)
    remaining = jnp.exp(last - total)
    erase_end = remaining * rate
    write_end = remaining * mixed
    final = jnp.exp(last)
    strict = row > col
    inclusive = row >= col
    hrow, hcol = iotas(CH, CH)
    every = range(w // CH)

    def parts(array):
        return [array[:, h * CH : (h + 1) * CH] for h in every]

    befores, asked, values = parts(before), parts(read), parts(value)
    pairs = [
        mm(jnp.concatenate([b, q], 0), jnp.concatenate([e, x], 0), NT)
        for b, q, e, x in zip(befores, asked, parts(erase), parts(write))
    ]
    lows = [jnp.where(strict, p[:t, :t], 0.0) for p in pairs]
    stacks = [
        jnp.concatenate(
            [jnp.where(strict, p[:t, t:], 0.0), jnp.where(inclusive, p[t:, t:], 0.0)], 0
        )
        for p in pairs
    ]
    on_values = [mm(stack, v) for stack, v in zip(stacks, values)]
    written = [mm(e, v, TN) for e, v in zip(parts(write_end), values)]
    xs = unit_inverses(lows)
    solved = [
        mm(x, jnp.concatenate([b, o[:t]], 1)) for x, b, o in zip(xs, befores, on_values)
    ]
    states = [mm(e, z, TN) for e, z in zip(parts(erase_end), solved)]
    reads = [mm(jnp.where(inclusive, p[t:, :t], 0.0), z) for p, z in zip(pairs, solved)]
    for h, f in zip(every, parts(final)):
        diagonal = jnp.where(hrow == hcol, jnp.broadcast_to(f, (CH, CH)), 0.0)
        state = states[h] + jnp.concatenate([diagonal, written[h]], 1)
        map_ref[2 * h], map_ref[2 * h + 1] = packed(state)
        read_ref[h] = reads[h] + jnp.concatenate([asked[h], on_values[h][t:]], 1)


def eye_of(width):
    row, col = iotas(CH, width)
    return jnp.where(row == col, 1.0, 0.0)


def folded(state, cols):
    half = CH // 2
    quarter = half // 2
    moved = state[:, :CH] - eye_of(CH)
    left = jnp.concatenate([moved[:half], moved[half:]], 1)
    rows = [state[i * quarter : (i + 1) * quarter, cols] for i in range(4)]
    return jnp.concatenate([left, jnp.concatenate(rows, 1)], 0).astype(BF16)


def packed(state):
    return [folded(state, slice(CH + c * CH // 2, CH + (c + 1) * CH // 2)) for c in range(2)]


def repacked(state):
    return folded(state, slice(CH, None))


def unpacked(block):
    half = CH // 2
    block = block.astype(F32)
    left = jnp.concatenate([block[:half, :CH], block[:half, CH:]], 0) + eye_of(CH)
    right = jnp.concatenate([block[half:, i * half : (i + 1) * half] for i in range(4)], 0)
    return jnp.concatenate([left, right], 1)


def joined(former, latter, late):
    return mm(latter[:, :CH], former) + jnp.where(late, latter, 0.0)


def plane_kernel(map_ref, before_ref, total_ref):
    count = map_ref.shape[0]
    hrow, hcol = iotas(CH, 3 * CH // 2)
    late = hcol >= CH
    maps = [unpacked(map_ref[q]) for q in range(count)]
    span = 1
    while span < count:
        maps = [
            maps[q] if q < span else joined(maps[q - span], maps[q], late) for q in range(count)
        ]
        span *= 2
    total = repacked(maps[count - 1])
    for z in range(total_ref.shape[0]):
        total_ref[z] = total
    before_ref[0] = jnp.where(hrow == hcol, 1.0, 0.0)
    for q in range(1, count):
        before_ref[q] = maps[q - 1]


def entering_kernel(place_ref, before_ref, total_ref, out_ref):
    z_here = place_ref[0]
    hrow, hcol = iotas(CH, 3 * CH // 2)
    late = hcol >= CH
    nothing = jnp.where(hrow == hcol, 1.0, 0.0)
    maps = [
        jnp.where(z < z_here, unpacked(total_ref[z]), nothing)
        for z in range(total_ref.shape[0] - 1)
    ]
    while len(maps) > 1:
        odd = maps[:1] if len(maps) % 2 else []
        rest = maps[len(odd) :]
        maps = odd + [
            joined(rest[i], rest[i + 1], late) for i in range(0, len(rest), 2)
        ]
    state = maps[0][:, CH:]
    count = before_ref.shape[0]
    rows = jnp.concatenate([before_ref[q] for q in range(count)], 0)
    mine = mm(rows[:, :CH], state) + rows[:, CH:]
    quarter = CH // 4
    for q in range(count):
        pieces = [mine[q * CH + i * quarter : q * CH + (i + 1) * quarter] for i in range(4)]
        out_ref[q] = jnp.concatenate(pieces, 1).astype(BF16)


def finish_kernel(
    state_ref, read_ref, r_ref, k_ref, v_ref, c_ref, f_ref, mix_ref, cur_ref, gain_ref, bias_ref,
    out_ref,
):
    every = range(read_ref.shape[0])
    slices = [slice(h * CH, (h + 1) * CH) for h in every]
    mixed = mixed_of(k_ref[...].astype(F32), sigmoid(c_ref[...].astype(F32)), mix_ref[...])
    weight = r_ref[...].astype(F32) * mixed * cur_ref[...]
    readouts = []
    for h in every:
        even, odd = state_ref[2 * h].astype(F32), state_ref[2 * h + 1].astype(F32)
        half = CH // 2
        state = jnp.concatenate(
            [
                jnp.concatenate([ref[:, i * half : (i + 1) * half] for i in range(4)], 0)
                for ref in (even, odd)
            ],
            1,
        )
        reads = read_ref[h]
        readouts.append(reads[:, CH:] + mm(reads[:, :CH], state))
    bonuses = [jnp.sum(weight[:, s], axis=1, keepdims=True) for s in slices]
    means = [jnp.mean(readout, axis=1, keepdims=True) for readout in readouts]
    centred = [readout - mean for readout, mean in zip(readouts, means)]
    spreads = [jnp.mean(c * c, axis=1, keepdims=True) for c in centred]
    scaled = [c * lax.rsqrt(spread + GROUP_EPS) for c, spread in zip(centred, spreads)]
    wide = (readouts[0].shape[0], CH)
    bonus = jnp.concatenate([jnp.broadcast_to(b, wide) for b in bonuses], 1)
    grouped = jnp.concatenate(scaled, 1) * gain_ref[...] + bias_ref[...]
    out = (grouped + bonus * v_ref[...].astype(F32)) * f_ref[...].astype(F32)
    out_ref[...] = out.astype(BF16)


def project_kernel(
    place_ref, token_ref, h0_ref, h1_ref, h2_ref, h3_ref, gain_ref, own_ref, near_ref, far_ref, residual_ref, out_ref,
    normed_ref, own_middle_ref, wide_ref, rows_ref,
):
    core = place_ref[1]
    tp = place_ref[2]
    half = near_ref.shape[1]
    width = residual_ref.shape[1]
    heads = [h0_ref[...]]
    for ref in (h1_ref, h2_ref, h3_ref):
        head = ref[...]
        low, high = head[:, :half], head[:, half:]
        heads += [jnp.where(core == 0, low, high), jnp.where(core == 0, high, low)]
    heads = jnp.concatenate(heads, 1)
    pieces = []
    squares = jnp.zeros((heads.shape[0], LANES), F32)
    step = 2 * LANES
    for start in range(0, width, step):
        s = slice(start, start + step)
        rows = [own_ref[:, s]]
        for k in range(3):
            rows += [near_ref[k, :, s], far_ref[k, :, s]]
        acc = residual_ref[:, s].astype(F32) + dot(heads, jnp.concatenate(rows, 0))
        piece = acc.astype(BF16)
        full = piece.astype(F32)
        squares = squares + full[:, :LANES] * full[:, :LANES] + full[:, LANES:] * full[:, LANES:]
        pieces.append(piece)
    middle = jnp.concatenate(pieces, 1)
    full = middle.astype(F32)
    scale = lax.rsqrt(jnp.sum(squares, axis=1, keepdims=True) / width + NORM_EPS)
    normed = (full * scale * gain_ref[...]).astype(BF16)
    normed_ref[...] = normed
    cols = own_middle_ref.shape[1]
    own = middle[:, :cols]
    for y in range(1, middle.shape[1] // cols):
        own = jnp.where(tp == y, middle[:, y * cols : (y + 1) * cols], own)
    own_middle_ref[...] = own
    tiles = normed.shape[1] // LANES
    wide = normed.astype(F32)
    for i in range(tiles):
        wide_ref[:, i, :] = wide[:, i * LANES : (i + 1) * LANES]
    rows_ref[...] = wide_ref[:, :tiles, :].astype(BF16)
    dests = out_ref.shape[0] // (CAP * tiles)

    def send(i, carry):
        for m in range(CAP):
            token = jnp.maximum(token_ref[m, i * 4 + tp], 0)
            place = pl.multiple_of((i * CAP + m) * tiles, tiles)
            out_ref[pl.ds(place, tiles), :] = rows_ref[token]
        return carry

    lax.fori_loop(0, dests, send, 0, unroll=4)


def shared_kernel(place_ref, normed_ref, gate_ref, up_ref, down_ref, s0_ref, s1_ref, s2_ref, s3_ref):
    tp = place_ref[2]
    gate = dot(normed_ref[...], gate_ref[...])
    up = dot(normed_ref[...], up_ref[...])
    hidden = (gate * sigmoid(gate) * up).astype(BF16)
    cols = s0_ref.shape[1]
    for k, ref in enumerate((s0_ref, s1_ref, s2_ref, s3_ref)):
        start = pl.multiple_of(lax.rem(tp + k, 4) * cols, cols)
        ref[...] = dot(hidden, down_ref[:, pl.ds(start, cols)]).astype(ref.dtype)


def expert_kernel(rows_ref, gate_ref, up_ref, down_ref, out_ref, wide_ref, x_ref):
    width = gate_ref.shape[0]
    tiles = width // LANES
    block = CAP * tiles
    sources = rows_ref.shape[0] // block

    def widen(i, carry):
        wide_ref[pl.ds(pl.multiple_of(i * PAD, 8), block), :] = rows_ref[
            pl.ds(pl.multiple_of(i * block, block), block), :
        ].astype(F32)
        return carry

    lax.fori_loop(0, sources, widen, 0, unroll=4)
    for m in range(CAP):
        for i in range(tiles):
            x_ref[m * sources : (m + 1) * sources, i * LANES : (i + 1) * LANES] = wide_ref[
                pl.ds(m * tiles + i, sources, stride=PAD), :
            ].astype(BF16)
    x = x_ref[...]
    gate = dot(x, gate_ref[...])
    up = dot(x, up_ref[...])
    hidden = (gate * sigmoid(gate) * up).astype(BF16)
    cols = width // 4
    for y in range(4):
        answer = dot(hidden, down_ref[:, y * cols : (y + 1) * cols])
        for m in range(CAP):
            for i in range(cols // LANES):
                place = (y * CAP + m) * (cols // LANES) + i
                wide_ref[pl.ds(place, sources, stride=PAD), :] = answer[
                    m * sources : (m + 1) * sources, i * LANES : (i + 1) * LANES
                ]

    def narrow(i, carry):
        out_ref[pl.ds(pl.multiple_of(i * block, block), block), :] = wide_ref[
            pl.ds(pl.multiple_of(i * PAD, 8), block), :
        ].astype(BF16)
        return carry

    lax.fori_loop(0, sources, narrow, 0, unroll=4)


def combine_kernel(
    back_ref, token_ref, weight_ref, middle_ref, s0_ref, s1_ref, s2_ref, s3_ref, out_ref, wide_ref
):
    tokens, cols = out_ref.shape
    tiles = cols // LANES
    slots, experts = token_ref.shape
    wide_ref[...] = back_ref[...].astype(F32)
    token, _ = iotas(tokens, experts)
    total = middle_ref[...].astype(F32) + s0_ref[...] + s1_ref[...].astype(F32)
    total = total + s2_ref[...].astype(F32) + s3_ref[...].astype(F32)
    tables, rows = [], []
    for m in range(slots):
        same = token_ref[m : m + 1, :] == token
        tables.append(jnp.where(same, weight_ref[m : m + 1, :], 0.0).astype(BF16))
        rows.append(
            jnp.concatenate(
                [
                    wide_ref[pl.ds(m * tiles + i, experts, stride=slots * tiles), :].astype(BF16)
                    for i in range(tiles)
                ],
                1,
            )
        )
    routed = dot(jnp.concatenate(tables, 1), jnp.concatenate(rows, 0))
    out_ref[...] = (total + routed).astype(BF16)


def call(kernel, out, *args, scalars=0, scratch=(), limit=16, inside=True, kept=True):
    smem = pl.BlockSpec(memory_space=pltpu.SMEM)
    vmem = pl.BlockSpec(memory_space=pltpu.VMEM)
    args = list(args)
    space = pltpu.VMEM if inside else pltpu.HBM
    args[scalars:] = [pltpu.with_memory_space_constraint(a, space) for a in args[scalars:]]
    return pl.pallas_call(
        kernel,
        out_shape=jax.tree.map(lambda a: pltpu.VMEM(a.shape, a.dtype), out) if kept else out,
        in_specs=[smem] * scalars + [vmem] * (len(args) - scalars),
        out_specs=jax.tree.map(lambda _: vmem, out),
        scratch_shapes=list(scratch),
        compiler_params=pltpu.CompilerParams(vmem_limit_bytes=limit << 20),
    )(*args)


def exchange(array, axes):
    return lax.all_to_all(array, axes, split_axis=0, concat_axis=0, tiled=True)


def turned(array, axis, shift):
    peers = lax.axis_size(axis)
    return lax.ppermute(array, axis, [(i, (i + shift) % peers) for i in range(peers)])


def layer(
    receptance, key, value, decay, correction, factor, mix, current, gain, bias, output_matrix,
    residual, norm_gain, routes, chosen, routed_gate, routed_up, routed_down, common_gate,
    common_up, common_down,
):
    shape = jax.ShapeDtypeStruct
    tokens, inner = key.shape
    width = residual.shape[1]
    cols = width // 4
    heads = inner // CH
    z_count, plane = lax.axis_size("z"), lax.axis_size(PLANE)
    experts = lax.axis_size(EVERY)
    slots = lax.axis_size(SP) * CAP
    core = lax.axis_index("c")
    place = jnp.stack([lax.axis_index("z"), core, lax.axis_index("tp")]).astype(jnp.int32)
    mix, current, gain, bias = (a.reshape(1, -1) for a in (mix, current, gain, bias))

    maps, reads = call(
        local_kernel,
        (shape((2 * heads, 3 * CH // 4, 2 * CH), BF16), shape((heads, tokens, 2 * CH), F32)),
        receptance, key, value, decay, correction, mix, inside=False,
    )
    maps, output_rows = lax.optimization_barrier((maps, output_matrix))
    half = inner // 2
    maps = exchange(maps, PLANE)
    mine = lax.dynamic_slice_in_dim(output_rows, core * half, half, 0)
    near = [turned(mine, "tp", k) for k in (1, 2, 3)]
    before, totals = call(
        plane_kernel,
        (
            shape((plane, CH, 3 * CH // 2), F32),
            shape((z_count, 3 * CH // 4, 2 * CH), BF16),
        ),
        maps,
    )
    totals = exchange(totals, "z")
    slot_token, slot_weight = call(
        routing_kernel,
        (shape((CAP, experts), jnp.int32), shape((CAP, experts), F32)), routes, chosen,
    )
    states = call(
        entering_kernel, shape((plane, CH // 4, 2 * CH), BF16), place, before, totals,
        scalars=1,
    )
    states = exchange(states, PLANE)
    states, *near = lax.optimization_barrier((states, *near))
    near = jnp.stack(near)
    far = turned(near, "c", 1)
    mixed = call(
        finish_kernel, shape((tokens, inner), BF16), states, reads, receptance, key,
        value, correction, factor, mix, current, gain, bias,
    )
    others = [turned(mixed, "tp", k) for k in (1, 2, 3)]
    outgoing, normed, own_middle = call(
        project_kernel,
        (
            shape((slots * width // LANES, LANES), BF16),
            shape((tokens, width), BF16),
            shape((tokens, cols), BF16),
        ),
        place, slot_token, mixed, *others, norm_gain.reshape(1, -1), output_matrix, near, far, residual,
        scalars=2,
        scratch=(
            pltpu.VMEM((tokens, width // LANES + 8, LANES), F32),
            pltpu.VMEM((tokens, width // LANES, LANES), BF16),
        ),
    )
    arrived = exchange(outgoing, SP)
    shared = call(
        shared_kernel,
        (shape((tokens, cols), F32),) + (shape((tokens, cols), BF16),) * 3,
        place, normed, common_gate, common_up, common_down, scalars=1,
    )
    shared = [shared[0]] + [turned(shared[k], "tp", k) for k in (1, 2, 3)]
    answer = call(
        expert_kernel, shape(outgoing.shape, BF16), arrived, routed_gate[0],
        routed_up[0], routed_down[0],
        scratch=(
            pltpu.VMEM((slots // CAP * PAD, LANES), F32),
            pltpu.VMEM((slots, width), BF16),
        ),
    )
    back = exchange(answer, EVERY)
    return call(
        combine_kernel, shape((tokens, cols), BF16), back, slot_token, slot_weight,
        own_middle, *shared,
        scratch=(pltpu.VMEM(back.shape, F32),), kept=False,
    )


def solution(mesh):
    finer = Mesh(mesh.devices.reshape(8, 4, 2, mesh.shape["tp"]), EVERY)
    placed = (
        (P(SP, "tp"),) * 6
        + (P("tp"),) * 4
        + (P("tp", None), P(SP, None), P(), P(SP, None), P(SP, None))
        + (P(EVERY, None, None),) * 3
        + (P(None, "tp"), P(None, "tp"), P("tp", None))
    )
    return jax.shard_map(layer, mesh=finer, in_specs=placed, out_specs=P(SP, "tp"), check_vma=False)
```

```python
import jax
import jax.numpy as jnp
from jax import lax
from jax.experimental import pallas as pl
from jax.experimental.pallas import tpu as pltpu
from jax.sharding import Mesh
from jax.sharding import PartitionSpec as P


CH = 64
CAP = 6
LANES = 128
NORM_EPS = 1e-06
GROUP_EPS = 0.00064
PLANE = ("x", "c")
SP = ("z", "x", "c")
EVERY = ("z", "x", "c", "tp")
F32 = jnp.float32
BF16 = jnp.bfloat16
NN = ((1,), (0,))
NT = ((1,), (1,))
TN = ((0,), (0,))
PAD = 104


def dot(a, b, dims=NN):
    return lax.dot_general(a, b, (dims, ((), ())), preferred_element_type=F32)


def split(a):
    high = a.astype(BF16)
    return high, (a - high.astype(F32)).astype(BF16)


def mm(a, b, dims=NN):
    ah, al = split(a)
    bh, bl = split(b)
    return dot(ah, bh, dims) + (dot(al, bh, dims) + dot(ah, bl, dims))


def iotas(rows, cols):
    return (
        lax.broadcasted_iota(jnp.int32, (rows, cols), 0),
        lax.broadcasted_iota(jnp.int32, (rows, cols), 1),
    )


def sigmoid(x):
    return 1.0 / (1.0 + jnp.exp(-x))


def unit_inverses(lows):
    n = lows[0].shape[0]
    row, col = iotas(n, n)
    size = 8
    eye = jnp.where(row == col, 1.0, 0.0)
    inside = (row // size) == (col // size)
    powers = [jnp.where(inside, low, 0.0) for low in lows]
    xs = [eye + power for power in powers]
    span = 2
    while span < size:
        powers = [mm(power, power) for power in powers]
        xs = [x + mm(x, power) for x, power in zip(xs, powers)]
        span *= 2
    while size < n:
        part = ((row // (2 * size)) == (col // (2 * size))) & ((row // size) != (col // size))
        lefts = [mm(x, jnp.where(part, low, 0.0)) for x, low in zip(xs, lows)]
        xs = [x + mm(left, x) for x, left in zip(xs, lefts)]
        size *= 2
    return xs


def mixed_of(key, learning, mix):
    return key * (1.0 + (learning - 1.0) * mix)


def routing_kernel(routes_ref, weight_ref, token_ref, slot_weight_ref):
    slots, experts = token_ref.shape
    tokens, top = routes_ref.shape
    token, expert = iotas(tokens, experts)
    weight = jnp.zeros((tokens, experts), F32)
    hit = jnp.zeros((tokens, experts), F32)
    for k in range(top):
        same = routes_ref[:, k : k + 1] == expert
        hit = jnp.where(same, 1.0, hit)
        weight = jnp.where(same, weight_ref[:, k : k + 1], weight)
    row, col = iotas(tokens, tokens)
    earlier = jnp.where(row > col, 1.0, 0.0).astype(BF16)
    within = dot(earlier, hit.astype(BF16))
    within = jnp.where(hit > 0.5, within, -1.0)
    number = token.astype(F32) + 1.0
    for m in range(slots):
        chosen = within == float(m)
        name = jnp.sum(jnp.where(chosen, number, 0.0), axis=0, keepdims=True) - 1.0
        token_ref[m : m + 1, :] = name.astype(jnp.int32)
        slot_weight_ref[m : m + 1, :] = jnp.sum(
            jnp.where(chosen, weight, 0.0), axis=0, keepdims=True
        )


def local_kernel(r_ref, k_ref, v_ref, d_ref, c_ref, mix_ref, map_ref, read_ref):
    t, w = k_ref.shape
    key = k_ref[...].astype(F32)
    learning = sigmoid(c_ref[...].astype(F32))
    log_decay = -0.6065306597126334 * sigmoid(d_ref[...].astype(F32))
    row, col = iotas(w, w)
    group = jnp.where(row // CH == col // CH, 1.0, 0.0).astype(BF16)
    square_high, square_low = split(key * key)
    length = jnp.sqrt(dot(square_high, group) + dot(square_low, group))
    unit = key / jnp.maximum(length, 1.0)
    mixed = mixed_of(key, learning, mix_ref[...])
    row, col = iotas(t, t)
    upto = jnp.where(row >= col, 1.0, 0.0).astype(BF16)
    first = log_decay.astype(BF16)
    second, third = split(log_decay - first.astype(F32))
    total = dot(upto, first) + (dot(upto, second) + dot(upto, third))
    last = total[t - 1 : t, :]
    value = v_ref[...].astype(F32)
    before = -jnp.exp(total - log_decay) * unit
    inverse_decay = jnp.exp(-total)
    rate = unit * learning
    erase = inverse_decay * rate
    write = inverse_decay * mixed
    read = jnp.exp(total) * r_ref[...].astype(F32)
    remaining = jnp.exp(last - total)
    erase_end = remaining * rate
    write_end = remaining * mixed
    final = jnp.exp(last)
    strict = row > col
    inclusive = row >= col
    hrow, hcol = iotas(CH, CH)
    every = range(w // CH)

    def parts(array):
        return [array[:, h * CH : (h + 1) * CH] for h in every]

    befores, asked, values = parts(before), parts(read), parts(value)
    pairs = [
        mm(jnp.concatenate([b, q], 0), jnp.concatenate([e, x], 0), NT)
        for b, q, e, x in zip(befores, asked, parts(erase), parts(write))
    ]
    lows = [jnp.where(strict, p[:t, :t], 0.0) for p in pairs]
    stacks = [
        jnp.concatenate(
            [jnp.where(strict, p[:t, t:], 0.0), jnp.where(inclusive, p[t:, t:], 0.0)], 0
        )
        for p in pairs
    ]
    on_values = [mm(stack, v) for stack, v in zip(stacks, values)]
    written = [mm(e, v, TN) for e, v in zip(parts(write_end), values)]
    xs = unit_inverses(lows)
    solved = [
        mm(x, jnp.concatenate([b, o[:t]], 1)) for x, b, o in zip(xs, befores, on_values)
    ]
    states = [mm(e, z, TN) for e, z in zip(parts(erase_end), solved)]
    reads = [mm(jnp.where(inclusive, p[t:, :t], 0.0), z) for p, z in zip(pairs, solved)]
    for h, f in zip(every, parts(final)):
        diagonal = jnp.where(hrow == hcol, jnp.broadcast_to(f, (CH, CH)), 0.0)
        state = states[h] + jnp.concatenate([diagonal, written[h]], 1)
        map_ref[2 * h], map_ref[2 * h + 1] = packed(state)
        read_ref[h] = reads[h] + jnp.concatenate([asked[h], on_values[h][t:]], 1)


def eye_of(width):
    row, col = iotas(CH, width)
    return jnp.where(row == col, 1.0, 0.0)


def folded(state, cols):
    half = CH // 2
    quarter = half // 2
    moved = state[:, :CH] - eye_of(CH)
    left = jnp.concatenate([moved[:half], moved[half:]], 1)
    rows = [state[i * quarter : (i + 1) * quarter, cols] for i in range(4)]
    return jnp.concatenate([left, jnp.concatenate(rows, 1)], 0).astype(BF16)


def packed(state):
    return [folded(state, slice(CH + c * CH // 2, CH + (c + 1) * CH // 2)) for c in range(2)]


def repacked(state):
    return folded(state, slice(CH, None))


def unpacked(block):
    half = CH // 2
    block = block.astype(F32)
    left = jnp.concatenate([block[:half, :CH], block[:half, CH:]], 0) + eye_of(CH)
    right = jnp.concatenate([block[half:, i * half : (i + 1) * half] for i in range(4)], 0)
    return jnp.concatenate([left, right], 1)


def joined(former, latter, late):
    return mm(latter[:, :CH], former) + jnp.where(late, latter, 0.0)


def plane_kernel(map_ref, before_ref, total_ref):
    count = map_ref.shape[0]
    hrow, hcol = iotas(CH, 3 * CH // 2)
    late = hcol >= CH
    maps = [unpacked(map_ref[q]) for q in range(count)]
    span = 1
    while span < count:
        maps = [
            maps[q] if q < span else joined(maps[q - span], maps[q], late) for q in range(count)
        ]
        span *= 2
    total = repacked(maps[count - 1])
    for z in range(total_ref.shape[0]):
        total_ref[z] = total
    before_ref[0] = jnp.where(hrow == hcol, 1.0, 0.0)
    for q in range(1, count):
        before_ref[q] = maps[q - 1]


def entering_kernel(place_ref, before_ref, total_ref, out_ref):
    z_here = place_ref[0]
    hrow, hcol = iotas(CH, 3 * CH // 2)
    late = hcol >= CH
    nothing = jnp.where(hrow == hcol, 1.0, 0.0)
    maps = [
        jnp.where(z < z_here, unpacked(total_ref[z]), nothing)
        for z in range(total_ref.shape[0] - 1)
    ]
    while len(maps) > 1:
        odd = maps[:1] if len(maps) % 2 else []
        rest = maps[len(odd) :]
        maps = odd + [
            joined(rest[i], rest[i + 1], late) for i in range(0, len(rest), 2)
        ]
    state = maps[0][:, CH:]
    count = before_ref.shape[0]
    rows = jnp.concatenate([before_ref[q] for q in range(count)], 0)
    mine = mm(rows[:, :CH], state) + rows[:, CH:]
    quarter = CH // 4
    for q in range(count):
        pieces = [mine[q * CH + i * quarter : q * CH + (i + 1) * quarter] for i in range(4)]
        out_ref[q] = jnp.concatenate(pieces, 1).astype(BF16)


def finish_kernel(
    state_ref, read_ref, r_ref, k_ref, v_ref, c_ref, f_ref, mix_ref, cur_ref, gain_ref, bias_ref,
    out_ref,
):
    every = range(read_ref.shape[0])
    slices = [slice(h * CH, (h + 1) * CH) for h in every]
    mixed = mixed_of(k_ref[...].astype(F32), sigmoid(c_ref[...].astype(F32)), mix_ref[...])
    weight = r_ref[...].astype(F32) * mixed * cur_ref[...]
    readouts = []
    for h in every:
        even, odd = state_ref[2 * h].astype(F32), state_ref[2 * h + 1].astype(F32)
        half = CH // 2
        state = jnp.concatenate(
            [
                jnp.concatenate([ref[:, i * half : (i + 1) * half] for i in range(4)], 0)
                for ref in (even, odd)
            ],
            1,
        )
        reads = read_ref[h]
        readouts.append(reads[:, CH:] + mm(reads[:, :CH], state))
    bonuses = [jnp.sum(weight[:, s], axis=1, keepdims=True) for s in slices]
    means = [jnp.mean(readout, axis=1, keepdims=True) for readout in readouts]
    centred = [readout - mean for readout, mean in zip(readouts, means)]
    spreads = [jnp.mean(c * c, axis=1, keepdims=True) for c in centred]
    scaled = [c * lax.rsqrt(spread + GROUP_EPS) for c, spread in zip(centred, spreads)]
    wide = (readouts[0].shape[0], CH)
    bonus = jnp.concatenate([jnp.broadcast_to(b, wide) for b in bonuses], 1)
    grouped = jnp.concatenate(scaled, 1) * gain_ref[...] + bias_ref[...]
    out = (grouped + bonus * v_ref[...].astype(F32)) * f_ref[...].astype(F32)
    out_ref[...] = out.astype(BF16)


def project_kernel(
    place_ref, token_ref, h0_ref, h1_ref, h2_ref, h3_ref, gain_ref, own_ref, near_ref, far_ref, residual_ref, out_ref,
    normed_ref, own_middle_ref, wide_ref, rows_ref,
):
    core = place_ref[1]
    tp = place_ref[2]
    half = near_ref.shape[1]
    width = residual_ref.shape[1]
    heads = [h0_ref[...]]
    for ref in (h1_ref, h2_ref, h3_ref):
        head = ref[...]
        low, high = head[:, :half], head[:, half:]
        heads += [jnp.where(core == 0, low, high), jnp.where(core == 0, high, low)]
    heads = jnp.concatenate(heads, 1)
    pieces = []
    squares = jnp.zeros((heads.shape[0], LANES), F32)
    step = 2 * LANES
    for start in range(0, width, step):
        s = slice(start, start + step)
        rows = [own_ref[:, s]]
        for k in range(3):
            rows += [near_ref[k, :, s], far_ref[k, :, s]]
        acc = residual_ref[:, s].astype(F32) + dot(heads, jnp.concatenate(rows, 0))
        piece = acc.astype(BF16)
        full = piece.astype(F32)
        squares = squares + full[:, :LANES] * full[:, :LANES] + full[:, LANES:] * full[:, LANES:]
        pieces.append(piece)
    middle = jnp.concatenate(pieces, 1)
    full = middle.astype(F32)
    scale = lax.rsqrt(jnp.sum(squares, axis=1, keepdims=True) / width + NORM_EPS)
    normed = (full * scale * gain_ref[...]).astype(BF16)
    normed_ref[...] = normed
    cols = own_middle_ref.shape[1]
    own = middle[:, :cols]
    for y in range(1, middle.shape[1] // cols):
        own = jnp.where(tp == y, middle[:, y * cols : (y + 1) * cols], own)
    own_middle_ref[...] = own
    tiles = normed.shape[1] // LANES
    wide = normed.astype(F32)
    for i in range(tiles):
        wide_ref[:, i, :] = wide[:, i * LANES : (i + 1) * LANES]
    rows_ref[...] = wide_ref[:, :tiles, :].astype(BF16)
    dests = out_ref.shape[0] // (CAP * tiles)

    def send(i, carry):
        for m in range(CAP):
            token = jnp.maximum(token_ref[m, i * 4 + tp], 0)
            place = pl.multiple_of((i * CAP + m) * tiles, tiles)
            out_ref[pl.ds(place, tiles), :] = rows_ref[token]
        return carry

    lax.fori_loop(0, dests, send, 0, unroll=4)


def shared_kernel(place_ref, normed_ref, gate_ref, up_ref, down_ref, s0_ref, s1_ref, s2_ref, s3_ref):
    tp = place_ref[2]
    gate = dot(normed_ref[...], gate_ref[...])
    up = dot(normed_ref[...], up_ref[...])
    hidden = (gate * sigmoid(gate) * up).astype(BF16)
    cols = s0_ref.shape[1]
    for k, ref in enumerate((s0_ref, s1_ref, s2_ref, s3_ref)):
        start = pl.multiple_of(lax.rem(tp + k, 4) * cols, cols)
        ref[...] = dot(hidden, down_ref[:, pl.ds(start, cols)]).astype(ref.dtype)


def expert_kernel(rows_ref, gate_ref, up_ref, down_ref, out_ref, wide_ref, x_ref):
    width = gate_ref.shape[0]
    tiles = width // LANES
    block = CAP * tiles
    sources = rows_ref.shape[0] // block

    def widen(i, carry):
        wide_ref[pl.ds(pl.multiple_of(i * PAD, 8), block), :] = rows_ref[
            pl.ds(pl.multiple_of(i * block, block), block), :
        ].astype(F32)
        return carry

    lax.fori_loop(0, sources, widen, 0, unroll=4)
    for m in range(CAP):
        for i in range(tiles):
            x_ref[m * sources : (m + 1) * sources, i * LANES : (i + 1) * LANES] = wide_ref[
                pl.ds(m * tiles + i, sources, stride=PAD), :
            ].astype(BF16)
    x = x_ref[...]
    gate = dot(x, gate_ref[...])
    up = dot(x, up_ref[...])
    hidden = (gate * sigmoid(gate) * up).astype(BF16)
    cols = width // 4
    for y in range(4):
        answer = dot(hidden, down_ref[:, y * cols : (y + 1) * cols])
        for m in range(CAP):
            for i in range(cols // LANES):
                place = (y * CAP + m) * (cols // LANES) + i
                wide_ref[pl.ds(place, sources, stride=PAD), :] = answer[
                    m * sources : (m + 1) * sources, i * LANES : (i + 1) * LANES
                ]

    def narrow(i, carry):
        out_ref[pl.ds(pl.multiple_of(i * block, block), block), :] = wide_ref[
            pl.ds(pl.multiple_of(i * PAD, 8), block), :
        ].astype(BF16)
        return carry

    lax.fori_loop(0, sources, narrow, 0, unroll=4)


def combine_kernel(
    back_ref, token_ref, weight_ref, middle_ref, s0_ref, s1_ref, s2_ref, s3_ref, out_ref, wide_ref
):
    tokens, cols = out_ref.shape
    tiles = cols // LANES
    slots, experts = token_ref.shape
    wide_ref[...] = back_ref[...].astype(F32)
    token, _ = iotas(tokens, experts)
    total = middle_ref[...].astype(F32) + s0_ref[...] + s1_ref[...].astype(F32)
    total = total + s2_ref[...].astype(F32) + s3_ref[...].astype(F32)
    tables, rows = [], []
    for m in range(slots):
        same = token_ref[m : m + 1, :] == token
        tables.append(jnp.where(same, weight_ref[m : m + 1, :], 0.0).astype(BF16))
        rows.append(
            jnp.concatenate(
                [
                    wide_ref[pl.ds(m * tiles + i, experts, stride=slots * tiles), :].astype(BF16)
                    for i in range(tiles)
                ],
                1,
            )
        )
    routed = dot(jnp.concatenate(tables, 1), jnp.concatenate(rows, 0))
    out_ref[...] = (total + routed).astype(BF16)


def call(kernel, out, *args, scalars=0, scratch=(), limit=16, inside=True, kept=True):
    smem = pl.BlockSpec(memory_space=pltpu.SMEM)
    vmem = pl.BlockSpec(memory_space=pltpu.VMEM)
    args = list(args)
    space = pltpu.VMEM if inside else pltpu.HBM
    args[scalars:] = [pltpu.with_memory_space_constraint(a, space) for a in args[scalars:]]
    return pl.pallas_call(
        kernel,
        out_shape=jax.tree.map(lambda a: pltpu.VMEM(a.shape, a.dtype), out) if kept else out,
        in_specs=[smem] * scalars + [vmem] * (len(args) - scalars),
        out_specs=jax.tree.map(lambda _: vmem, out),
        scratch_shapes=list(scratch),
        compiler_params=pltpu.CompilerParams(vmem_limit_bytes=limit << 20),
    )(*args)


def exchange(array, axes):
    return lax.all_to_all(array, axes, split_axis=0, concat_axis=0, tiled=True)


def turned(array, axis, shift):
    peers = lax.axis_size(axis)
    return lax.ppermute(array, axis, [(i, (i + shift) % peers) for i in range(peers)])


def layer(
    receptance, key, value, decay, correction, factor, mix, current, gain, bias, output_matrix,
    residual, norm_gain, routes, chosen, routed_gate, routed_up, routed_down, common_gate,
    common_up, common_down,
):
    shape = jax.ShapeDtypeStruct
    tokens, inner = key.shape
    width = residual.shape[1]
    cols = width // 4
    heads = inner // CH
    z_count, plane = lax.axis_size("z"), lax.axis_size(PLANE)
    experts = lax.axis_size(EVERY)
    slots = lax.axis_size(SP) * CAP
    core = lax.axis_index("c")
    place = jnp.stack([lax.axis_index("z"), core, lax.axis_index("tp")]).astype(jnp.int32)
    mix, current, gain, bias = (a.reshape(1, -1) for a in (mix, current, gain, bias))

    maps, reads = call(
        local_kernel,
        (shape((2 * heads, 3 * CH // 4, 2 * CH), BF16), shape((heads, tokens, 2 * CH), F32)),
        receptance, key, value, decay, correction, mix, inside=False,
    )
    maps, output_rows = lax.optimization_barrier((maps, output_matrix))
    half = inner // 2
    maps = exchange(maps, PLANE)
    mine = lax.dynamic_slice_in_dim(output_rows, core * half, half, 0)
    near = [turned(mine, "tp", k) for k in (1, 2, 3)]
    before, totals = call(
        plane_kernel,
        (
            shape((plane, CH, 3 * CH // 2), F32),
            shape((z_count, 3 * CH // 4, 2 * CH), BF16),
        ),
        maps,
    )
    totals = exchange(totals, "z")
    slot_token, slot_weight = call(
        routing_kernel,
        (shape((CAP, experts), jnp.int32), shape((CAP, experts), F32)), routes, chosen,
    )
    states = call(
        entering_kernel, shape((plane, CH // 4, 2 * CH), BF16), place, before, totals,
        scalars=1,
    )
    states = exchange(states, PLANE)
    mixed = call(
        finish_kernel, shape((tokens, inner), BF16), states, reads, receptance, key,
        value, correction, factor, mix, current, gain, bias,
    )
    others = []
    for k in (1, 2, 3):
        others.append(turned(mixed, "tp", k))
    _, *near = lax.optimization_barrier((mixed, *near))
    near = jnp.stack(near)
    far = turned(near, "c", 1)
    outgoing, normed, own_middle = call(
        project_kernel,
        (
            shape((slots * width // LANES, LANES), BF16),
            shape((tokens, width), BF16),
            shape((tokens, cols), BF16),
        ),
        place, slot_token, mixed, *others, norm_gain.reshape(1, -1), output_matrix, near, far, residual,
        scalars=2,
        scratch=(
            pltpu.VMEM((tokens, width // LANES + 8, LANES), F32),
            pltpu.VMEM((tokens, width // LANES, LANES), BF16),
        ),
    )
    arrived = exchange(outgoing, SP)
    shared = call(
        shared_kernel,
        (shape((tokens, cols), F32),) + (shape((tokens, cols), BF16),) * 3,
        place, normed, common_gate, common_up, common_down, scalars=1,
    )
    shared = [shared[0]] + [turned(shared[k], "tp", k) for k in (1, 2, 3)]
    answer = call(
        expert_kernel, shape(outgoing.shape, BF16), arrived, routed_gate[0],
        routed_up[0], routed_down[0],
        scratch=(
            pltpu.VMEM((slots // CAP * PAD, LANES), F32),
            pltpu.VMEM((slots, width), BF16),
        ),
    )
    back = exchange(answer, EVERY)
    return call(
        combine_kernel, shape((tokens, cols), BF16), back, slot_token, slot_weight,
        own_middle, *shared,
        scratch=(pltpu.VMEM(back.shape, F32),), kept=False,
    )


def solution(mesh):
    finer = Mesh(mesh.devices.reshape(8, 4, 2, mesh.shape["tp"]), EVERY)
    placed = (
        (P(SP, "tp"),) * 6
        + (P("tp"),) * 4
        + (P("tp", None), P(SP, None), P(), P(SP, None), P(SP, None))
        + (P(EVERY, None, None),) * 3
        + (P(None, "tp"), P(None, "tp"), P("tp", None))
    )
    return jax.shard_map(layer, mesh=finer, in_specs=placed, out_specs=P(SP, "tp"), check_vma=False)
```
